32 devices in a mesh: fs: 8 (over z, x), tp: 4 (over y, core).
Axes of the slice: x: 2, y: 2, z: 4, core: 2. Of those that a mesh axis runs over, the one named last changes fastest.
Arguments:
- tokens: bfloat16 [768, 4096], P('tp'), may hold values from -6 to 6
- norm_gain: float32 [4096], P('fs'), may hold values from 0.1 to 1.9
- gate_trained: float32 [4096, 11264], P('fs', 'tp'), may hold values from -0.09375 to 0.09375
- up_trained: float32 [4096, 11264], P('fs', 'tp'), may hold values from -0.09375 to 0.09375
- down_trained: float32 [11264, 4096], P('fs', 'tp'), may hold values from -0.078125 to 0.078125
Outputs:
- gate_sampler: bfloat16 [4096, 11264], P(None, 'fs')
- up_sampler: bfloat16 [4096, 11264], P(None, 'fs')
- down_sampler: bfloat16 [11264, 4096], P('fs')
- mixed_out: bfloat16 [768, 4096], P('tp', 'fs')
The draws below stay inside these ranges and needn't reach their ends.
All inputs are finite; a program needn't handle non-finite values.
Results may differ from the reference program's by a relative error of at most 0.0082.
Values may be sent and summed in bfloat16 or wider, within the bound.
A program may use at most 128 MiB of HBM per device.

```python
import jax
import jax.numpy as jnp
from jax import lax

D = 4096
FF = 11264
TOKENS = 768


def spiked(entries, own_key, source, target, shards_of, factor):
    def block_of(axis_at):
        return (jnp.arange(entries.shape[axis_at]) // (entries.shape[axis_at] // shards_of)).reshape((-1,) + (1,) * (entries.ndim - 1 - axis_at))

    first = jax.random.permutation(own_key, shards_of)[block_of(target)]
    second = (block_of(target) + shards_of // 2) % shards_of
    return jnp.where((block_of(source) == first) | (block_of(source) == second), factor * entries, entries)


def shard_levels(rng, dims, shards, least, largest):
    loudness, own = 1.0, jax.random.fold_in(rng, 6)
    for dim, blocks in shards:
        steps = jnp.exp(jax.random.uniform(jax.random.fold_in(own, dim), (blocks,), jnp.float32, least / len(shards), largest / len(shards)))
        loudness = loudness * jnp.repeat(steps, dims[dim] // blocks).reshape([-1 if axis == dim else 1 for axis in range(len(dims))])
    return loudness


def gaussian(own_key, shape, scale, limit, cuts=(), kind=jnp.bfloat16):
    array = scale * jax.random.normal(own_key, shape, jnp.float32)
    if cuts:
        array = array * shard_levels(own_key, shape, cuts, -0.22, 0.18)
    return jnp.clip(array, -limit, limit).astype(kind)


def gaussian_with(rng, shape, scale, reach, split, heavy, held_as=jnp.bfloat16):
    values = scale * jax.random.normal(rng, shape, jnp.float32)
    if split:
        values = values * shard_levels(rng, shape, split, -0.22, 0.18)
    return jnp.clip(spiked(values, jax.random.fold_in(rng, 3), *heavy), -reach, reach).astype(held_as)


def setup_inputs(seed: int = 0) -> dict:
    key_list = jax.random.split(jax.random.key(seed), 6)
    tokens = gaussian(key_list[0], (TOKENS, D), 1.0, 6.0, ((0, 4),))
    norm_gain = jnp.clip(1.0 + 0.18 * jax.random.normal(key_list[1], (D,), jnp.float32), 0.1, 1.9)
    gate_trained = gaussian(key_list[2], (D, FF), D ** -0.5, 0.09375, ((0, 8), (1, 4)), jnp.float32)
    up_trained = gaussian(key_list[3], (D, FF), D ** -0.5, 0.09375, ((0, 8), (1, 4)), jnp.float32)
    down_trained = gaussian_with(key_list[4], (FF, D), FF ** -0.5, 0.078125, ((0, 8), (1, 4)), (0, 1, 8, 2.0), jnp.float32)
    return {"tokens": tokens, "norm_gain": norm_gain, "gate_trained": gate_trained, "up_trained": up_trained, "down_trained": down_trained}


def reference(tokens, norm_gain, gate_trained, up_trained, down_trained):
    gate_sampler = (norm_gain[:, None] * gate_trained).astype(jnp.bfloat16)
    up_sampler = (norm_gain[:, None] * up_trained).astype(jnp.bfloat16)
    down_sampler = down_trained.astype(jnp.bfloat16)
    as_float = tokens.astype(jnp.float32)
    normed = (as_float * jax.lax.rsqrt(lax.optimization_barrier(jnp.mean(as_float * as_float, axis=-1, keepdims=True)) + 1e-06)).astype(jnp.bfloat16)
    gate_act = jnp.dot(normed, gate_sampler, preferred_element_type=jnp.float32)
    up_act = jnp.dot(normed, up_sampler, preferred_element_type=jnp.float32)
    hidden = (jax.nn.silu(gate_act) * up_act).astype(jnp.bfloat16)
    mixed_out = jnp.dot(hidden, down_sampler, preferred_element_type=jnp.float32).astype(jnp.bfloat16)
    return (gate_sampler, up_sampler, down_sampler, mixed_out)
```

```python
import functools

import jax
import jax.numpy as jnp
from jax import lax
from jax.experimental import pallas as pl
from jax.experimental.pallas import tpu as pltpu
from jax.sharding import PartitionSpec as P

MESH = pl.DeviceIdType.MESH


def handoff_kernel(
    slabs, fs_count, tp_count, chunks,
    gain_ref, tokens_ref, gate_in, up_in, down_in, *refs,
):
    outs, refs = refs[:2], refs[2:]
    down_out, own_out, refs = refs[0], refs[1], refs[2:]
    far_outs, refs = refs[:fs_count - 1], refs[fs_count - 1:]
    (
        land, land_down, own, stage, fbuf, dbuf, normed, act, hidden, own_buf, far_buf,
        fetch_sem, down_sem, token_sem, swap_send, swap_recv, own_send, pass_send, recv,
        core_send, core_recv, cross_send, cross_recv, dx_send, dx_recv, dc_send, dc_recv,
        dp_send, dp_recv, out_sem, down_out_sem, term_sem,
    ) = refs
    ins = (gate_in, up_in)
    blocks, _, rows, owned = own.shape
    down_rows, down_cols = dbuf.shape[1], down_in.shape[1]
    side = fs_count // 2
    single = slabs[0][1]
    cut = rows // 2
    count = len(slabs)
    early = [p for p in range(count) if slabs[p][0] < cut]
    late = [p for p in range(count) if slabs[p][0] >= cut]

    f = lax.axis_index("fs")
    t = lax.axis_index("tp")
    plane, core = lax.div(t, 2), lax.rem(t, 2)
    across = plane * -2 + 2 + core
    partner = plane * 2 + 1 - core
    far_partner = plane * -2 + 3 - core
    z = lax.div(f, blocks)
    half = lax.div(f, side)
    native = half == plane
    foreign = jnp.logical_not(native)
    held_here = lax.rem(z, 2) == core

    def remote(src, dst, send, sem, to):
        return pltpu.make_async_remote_copy(
            src_ref=src, dst_ref=dst, send_sem=send, recv_sem=sem, device_id=to,
            device_id_type=MESH,
        )

    def at(m, source, start, size):
        return land.at[m, pl.ds(pl.multiple_of(source * rows + start, 16), size), :]

    def columns(p):
        first = lax.rem(z + p, blocks)
        return [lax.rem(first + k, blocks) for k in range(blocks)]

    def key(p, j, m):
        return p * blocks * 2 + j * 2 + m

    def swap(p, j, m):
        start, size = slabs[p]
        there = pl.ds(start, size)
        return remote(
            own.at[j, m, there, :], stage.at[j, m, there, :],
            swap_send.at[key(p, j, m)], swap_recv.at[key(p, j, m)], (f, across),
        )

    def to_owner(held, sems, target, p, j, m):
        start, size = slabs[p]
        owner = target * blocks + j
        there = remote(
            held.at[j, m, pl.ds(start, size), :], at(m, f, start, size),
            sems.at[key(p, j, m)], recv.at[f, p], (owner, plane * 2 + m),
        )
        return there, jnp.logical_and(owner == f, core == m)

    def send_to_owner(held, sems, target, p, j, m):
        there, local = to_owner(held, sems, target, p, j, m)
        start, size = slabs[p]

        @pl.when(local)
        def _():
            @pl.loop(0, size // 16)
            def _(i):
                src = pl.ds(pl.multiple_of(start + i * 16, 16), 16)
                dst = pl.ds(pl.multiple_of(f * rows + start + i * 16, 16), 16)
                land[m, dst, :] = held[j, m, src, :]

        @pl.when(jnp.logical_not(local))
        def _():
            there.start()

    def wait_sent(held, sems, target, p, j, m):
        there, local = to_owner(held, sems, target, p, j, m)
        pl.when(jnp.logical_not(local))(there.wait_send)

    steps = [(p, m) for p in range(count) for m in range(2)]
    depth = fbuf.shape[0]

    def fetch(k):
        p, m = steps[k]
        start, size = slabs[p]
        return pltpu.make_async_copy(
            ins[m].at[pl.ds(start, size), :], fbuf.at[k % depth, pl.ds(0, size), :],
            fetch_sem.at[k % depth],
        )

    def down_fetch(q):
        return pltpu.make_async_copy(
            down_in.at[pl.ds(q * down_rows, down_rows), :], dbuf.at[q % 2], down_sem.at[q % 2]
        )

    def begin(p, m):
        for j in columns(p):
            def crossing(j=j):
                swap(p, j, m).start()

            def direct(j=j):
                send_to_owner(own, own_send, t, p, j, m)

            if p == 0:
                direct()
                pl.when(native)(crossing)
            elif p == 1:
                crossing()
                pl.when(native)(direct)
            else:
                crossing()

    for k in range(depth):
        fetch(k).start()
    token_copy = pltpu.make_async_copy(tokens_ref, normed, token_sem)
    token_copy.start()
    for k, (p, m) in enumerate(steps):
        start, size = slabs[p]
        fetch(k).wait()

        @pl.loop(0, size // 16)
        def _(i):
            src = pl.ds(pl.multiple_of(i * 16, 16), 16)
            dst = pl.ds(pl.multiple_of(start + i * 16, 16), 16)
            gain = gain_ref[dst, :]
            for j in range(blocks):
                own[j, m, dst, :] = (
                    gain * fbuf[k % depth, src, j * owned:(j + 1) * owned]
                ).astype(jnp.bfloat16)

        if k + depth < len(steps):
            fetch(k + depth).start()
        if k:
            begin(*steps[k - 1])
    for q in range(min(2, chunks)):
        down_fetch(q).start()
    begin(*steps[-1])

    def down_at(which, q):
        return land_down.at[
            pl.ds(q * down_rows, down_rows),
            pl.ds(pl.multiple_of(which * down_cols, 128), down_cols),
        ]

    for q in range(chunks):
        down_fetch(q).wait()

        @pl.loop(0, down_rows // 16)
        def _(i):
            src = pl.ds(pl.multiple_of(i * 16, 16), 16)
            dst = pl.ds(pl.multiple_of(q * down_rows + i * 16, 16), 16)
            land_down[dst, pl.ds(pl.multiple_of(t * down_cols, 128), down_cols)] = (
                dbuf[q % 2, src, :].astype(jnp.bfloat16)
            )

        if q + 2 < chunks:
            down_fetch(q + 2).start()

    token_copy.wait()

    @pl.loop(0, normed.shape[0] // 16)
    def _(i):
        dst = pl.ds(pl.multiple_of(i * 16, 16), 16)
        value = normed[dst, :].astype(jnp.float32)
        scale = lax.rsqrt(jnp.mean(value * value, axis=-1, keepdims=True) + 1e-06)
        normed[dst, :] = (value * scale).astype(jnp.bfloat16)
        for m in range(2):
            act[m, dst, :] = jnp.zeros((16, owned), jnp.float32)

    near_p = jnp.where(native, 0, 1)
    far_p = 1 - near_p

    def other(i):
        return (1 - half) * side + lax.rem(f + i, side)

    def same(i):
        return half * side + lax.rem(f + i, side)

    def to_partner(source, p, start, size):
        here = at(core, source, start, size)
        return remote(
            here, here, core_send.at[source, p], core_recv.at[source, p], (f, partner)
        )

    def from_partner(source, p, start, size):
        here = at(1 - core, source, start, size)
        return remote(
            here, here, core_send.at[source, p], core_recv.at[source, p], (f, partner)
        )

    def arrived(source, p, start, size):
        here = at(core, source, start, size)
        return remote(here, here, core_send.at[source, p], recv.at[source, p], (f, partner))

    def crossed(source, which):
        here = at(core, source, which * single, single)
        return remote(
            here, here, cross_send.at[source], cross_recv.at[source], (f, across)
        )

    def cross_near():
        @pl.loop(0, side)
        def _(i):
            source = other(i)
            arrived(source, near_p, near_p * single, single).wait_recv()
            crossed(source, near_p).start()
            to_partner(source, near_p, near_p * single, single).start()

    def down_cross(q):
        return remote(down_at(t, q), down_at(t, q), dx_send.at[q], dx_recv.at[q], (f, across))

    def down_core(which, q):
        return remote(
            down_at(which, q), down_at(which, q), dc_send.at[q], dc_recv.at[q], (f, partner)
        )

    def down_pass(which, q):
        return remote(
            down_at(which, q), down_at(which, q), dp_send.at[q], dp_recv.at[q], (f, partner)
        )

    def forward(p):
        for j in columns(p):
            for m in range(2):
                swap(p, j, m).wait_recv()
                send_to_owner(stage, pass_send, across, p, j, m)

    turn = count - 3
    for p in range(count):
        if p == 0:
            pl.when(foreign)(functools.partial(forward, p))
        else:
            forward(p)
        if 2 + p < count:
            for j in columns(2 + p):
                for m in range(2):
                    send_to_owner(own, own_send, t, 2 + p, j, m)
        if p == turn:
            cross_near()
            for q in range(chunks):
                down_cross(q).start()
                down_core(t, q).start()

    def take(source, p):
        start, size = slabs[p]
        pl.when(jnp.logical_not(jnp.logical_and(source == f, held_here)))(
            arrived(source, p, start, size).wait_recv
        )
        to_partner(source, p, start, size).start()

    def multiply(source, lo, size):
        lanes = pl.ds(pl.multiple_of(source * rows + lo, 128), size)
        left = normed[:, lanes]
        for m in range(2):
            act[m] += jnp.dot(
                left, land[m, pl.ds(pl.multiple_of(source * rows + lo, 16), size), :],
                preferred_element_type=jnp.float32,
            )

    def out_copy(source, m):
        here = pl.ds(pl.multiple_of(source * rows, 16), rows)
        return pltpu.make_async_copy(land.at[m, here, :], outs[m].at[here, :], out_sem.at[source, m])

    @pl.loop(0, side)
    def _(i):
        for p in early:
            take(same(i), p)

    @pl.loop(0, side)
    def _(i):
        for p in early[2:]:
            take(other(i), p)

    @pl.loop(0, side)
    def _(i):
        source = other(i)
        crossed(source, far_p).wait_recv()
        to_partner(source, far_p, far_p * single, single).start()

    @pl.loop(0, fs_count)
    def _(i):
        source = lax.rem(half * side + i, fs_count)
        for p in early:
            from_partner(source, p, *slabs[p]).wait_recv()
        multiply(source, 0, cut)

    def down_on(q):
        down_in_here = remote(
            down_at(across, q), down_at(across, q), dx_send.at[q], dx_recv.at[q], (f, across)
        )
        down_in_here.wait_recv()
        down_pass(across, q).start()

    def down_done(q):
        down_core(partner, q).wait_recv()
        down_pass(far_partner, q).wait_recv()
        here = pl.ds(q * down_rows, down_rows)
        return pltpu.make_async_copy(
            land_down.at[here, :], down_out.at[here, :], down_out_sem.at[q]
        )

    for n, p in enumerate(late[:-1]):
        @pl.loop(0, side)
        def _(i):
            take(same(i), p)

        @pl.loop(0, side)
        def _(i):
            take(other(i), p)

        if n < chunks - 2:
            down_on(n)
    last_p = late[-1]

    def finish(source):
        for p in late:
            from_partner(source, p, *slabs[p]).wait_recv()
        multiply(source, cut, rows - cut)
        for m in range(2):
            out_copy(source, m).start()

    @pl.loop(0, side)
    def _(i):
        take(same(i), last_p)

    @pl.loop(0, side)
    def _(i):
        finish(same(i))

    for q in range(len(late) - 1, chunks - 1):
        down_on(q)

    @pl.loop(0, side)
    def _(i):
        take(other(i), last_p)

        @pl.when(i > 0)
        def _():
            finish(other(i - 1))

    for q in range(max(0, chunks - 1), chunks):
        down_on(q)
    finish(other(side - 1))

    @pl.loop(0, normed.shape[0] // 16)
    def _(i):
        dst = pl.ds(pl.multiple_of(i * 16, 16), 16)
        gate = act[0, dst, :]
        small = jnp.exp(-jnp.abs(gate))
        silu = gate * jnp.where(gate >= 0, 1.0, small) / (1.0 + small)
        hidden[dst, :] = (silu * act[1, dst, :]).astype(jnp.bfloat16)

    for q in range(chunks):
        down_done(q).start()
    width = own_buf.shape[1]

    def term(b):
        lanes = pl.ds(pl.multiple_of(b * width, 128), width)
        return jnp.dot(hidden[...], land_down[:, lanes], preferred_element_type=jnp.float32)

    def put_term(k):
        if k == 0:
            return pltpu.make_async_copy(own_buf, own_out, term_sem.at[0])
        return pltpu.make_async_copy(far_buf.at[k - 1], far_outs[k - 1], term_sem.at[k])

    for k in range(1, fs_count):
        far_buf[k - 1] = term(lax.rem(f + k, fs_count)).astype(jnp.bfloat16)
        if k > 1:
            put_term(k - 1).start()
    own_buf[...] = term(f)
    put_term(fs_count - 1).start()

    for p in range(count):
        for j in range(blocks):
            for m in range(2):
                there = swap(p, j, m)
                if p == 0:
                    wait_sent(own, own_send, t, p, j, m)
                    pl.when(native)(there.wait_send)
                    pl.when(foreign)(
                        functools.partial(wait_sent, stage, pass_send, across, p, j, m)
                    )
                else:
                    there.wait_send()
                    wait_sent(stage, pass_send, across, p, j, m)
                    if p == 1:
                        pl.when(native)(functools.partial(wait_sent, own, own_send, t, p, j, m))
                    else:
                        wait_sent(own, own_send, t, p, j, m)
    put_term(0).start()

    @pl.loop(0, side)
    def _(i):
        crossed(other(i), near_p).wait_send()

    @pl.loop(0, fs_count)
    def _(i):
        for p in range(count):
            to_partner(i, p, *slabs[p]).wait_send()
        for m in range(2):
            out_copy(i, m).wait()

    for q in range(chunks):
        down_cross(q).wait_send()
        down_core(t, q).wait_send()
        down_pass(across, q).wait_send()
        here = pl.ds(q * down_rows, down_rows)
        pltpu.make_async_copy(
            land_down.at[here, :], down_out.at[here, :], down_out_sem.at[q]
        ).wait()
    for k in range(fs_count):
        put_term(k).wait()


def row_slabs(rows):
    single = max(16, (rows * 5 // 32) // 16 * 16)
    cut = rows // 2
    slabs = [(0, single), (single, single), (2 * single, cut - 2 * single)]
    left, start = (rows - cut) // 16, cut
    for k in range(3):
        size = -(-left // (3 - k)) * 16
        slabs.append((start, size))
        start, left = start + size, left - size // 16
    return slabs


def handoff(fs_count, tp_count, chunks, tokens, norm_gain, gate, up, down):
    rows, cols = gate.shape
    blocks = fs_count // tp_count
    owned = cols // blocks
    width = down.shape[1] * tp_count // fs_count
    down_rows, down_cols = down.shape
    model = rows * fs_count
    count = tokens.shape[0]
    slabs = row_slabs(rows)
    parts = len(slabs)
    f32, bf16, dma = jnp.float32, jnp.bfloat16, pltpu.SemaphoreType.DMA
    anywhere = pl.BlockSpec(memory_space=pl.ANY)
    tall = max(size for _, size in slabs)
    pieces = parts * blocks * 2
    return pl.pallas_call(
        functools.partial(handoff_kernel, slabs, fs_count, tp_count, chunks),
        out_shape=[
            jax.ShapeDtypeStruct((model, owned), bf16),
            jax.ShapeDtypeStruct((model, owned), bf16),
            jax.ShapeDtypeStruct((down_rows, down_cols * tp_count), bf16),
            jax.ShapeDtypeStruct((count, width), f32),
        ] + [jax.ShapeDtypeStruct((count, width), bf16)] * (fs_count - 1),
        in_specs=[pl.BlockSpec(memory_space=pltpu.VMEM)] + [anywhere] * 4,
        out_specs=[anywhere] * (3 + fs_count),
        scratch_shapes=[
            pltpu.VMEM((2, model, owned), bf16),
            pltpu.VMEM((down_rows, down_cols * tp_count), bf16),
            pltpu.VMEM((blocks, 2, rows, owned), bf16),
            pltpu.VMEM((blocks, 2, rows, owned), bf16),
            pltpu.VMEM((3, tall, cols), f32),
            pltpu.VMEM((2, down_rows // chunks, down_cols), f32),
            pltpu.VMEM(tokens.shape, bf16),
            pltpu.VMEM((2, count, owned), f32),
            pltpu.VMEM((count, owned), bf16),
            pltpu.VMEM((count, width), f32),
            pltpu.VMEM((fs_count - 1, count, width), bf16),
            dma((3,)), dma((2,)), dma(()),
            dma((pieces,)), dma((pieces,)), dma((pieces,)), dma((pieces,)),
            dma((fs_count, parts)), dma((fs_count, parts)), dma((fs_count, parts)),
            dma((fs_count,)), dma((fs_count,)),
            dma((chunks,)), dma((chunks,)), dma((chunks,)), dma((chunks,)),
            dma((chunks,)), dma((chunks,)),
            dma((fs_count, 2)), dma((chunks,)), dma((fs_count,)),
        ],
        compiler_params=pltpu.CompilerParams(
            has_side_effects=True, vmem_limit_bytes=62 * 1024 * 1024
        ),
    )(norm_gain[:, None], tokens, gate, up, down)


def put_out(landed):
    rows, cols = landed.shape
    step = max(r for r in range(16, min(rows, 512) + 1, 16) if rows % r == 0)

    def copy_kernel(in_ref, out_ref):
        out_ref[...] = in_ref[...]

    spec = pl.BlockSpec((step, cols), lambda i: (i, 0))
    return pl.pallas_call(
        copy_kernel,
        grid=(rows // step,),
        out_shape=jax.ShapeDtypeStruct(landed.shape, landed.dtype),
        in_specs=[spec],
        out_specs=spec,
        cost_estimate=pl.CostEstimate(
            flops=0, bytes_accessed=2 * landed.size * landed.dtype.itemsize, transcendentals=0
        ),
    )(landed)


def scatter_sum(own, far, fs_count):
    arrived = []
    for k in range(1, fs_count):
        ring = [(i, (i + k) % fs_count) for i in range(fs_count)]
        arrived.append(lax.ppermute(far[k - 1], "fs", ring))
    total = own
    for piece in arrived:
        total = total + piece.astype(jnp.float32)
    return total.astype(jnp.bfloat16)


def per_device(tokens, norm_gain, gate_trained, up_trained, down_trained):
    tp_count = lax.axis_size("tp")
    fs_count = lax.axis_size("fs")
    gate_sampler, up_sampler, down_sampler, own, *far = handoff(
        fs_count, tp_count, 4, tokens, norm_gain, gate_trained, up_trained, down_trained
    )
    return (
        put_out(gate_sampler), put_out(up_sampler), put_out(down_sampler),
        scatter_sum(own, far, fs_count),
    )


def per_device_plain(tokens, norm_gain, gate_trained, up_trained, down_trained):
    gate_local = (norm_gain[:, None] * gate_trained).astype(jnp.bfloat16)
    up_local = (norm_gain[:, None] * up_trained).astype(jnp.bfloat16)
    down_local = down_trained.astype(jnp.bfloat16)
    tp_count = lax.axis_size("tp")
    fs_count = lax.axis_size("fs")
    rows_local = gate_local.shape[0]
    cols_local = gate_local.shape[1]
    model_width = rows_local * fs_count
    owned_count = cols_local * tp_count // fs_count
    piece_cols = owned_count // tp_count
    block_count = cols_local // owned_count

    def arrange(matrix):
        return matrix.reshape(rows_local, block_count, tp_count, piece_cols)

    gate_mixed, up_mixed = (
        lax.all_to_all(arrange(gate_local), "tp", split_axis=2, concat_axis=2, tiled=True),
        lax.all_to_all(arrange(up_local), "tp", split_axis=2, concat_axis=2, tiled=True),
    )

    def regroup(matrix):
        return matrix.transpose(2, 1, 0, 3).reshape(fs_count, rows_local, piece_cols)

    gate_parts, up_parts = (
        lax.all_to_all(regroup(gate_mixed), "fs", split_axis=0, concat_axis=1, tiled=True),
        lax.all_to_all(regroup(up_mixed), "fs", split_axis=0, concat_axis=1, tiled=True),
    )
    gate_sampler, up_sampler, down_sampler = (
        lax.all_gather(gate_parts.reshape(model_width, piece_cols), "tp", axis=1, tiled=True),
        lax.all_gather(up_parts.reshape(model_width, piece_cols), "tp", axis=1, tiled=True),
        lax.all_gather(down_local, "tp", axis=1, tiled=True),
    )
    as_float = tokens.astype(jnp.float32)
    normed = (
        as_float * lax.rsqrt(jnp.mean(as_float * as_float, axis=-1, keepdims=True) + 1e-06)
    ).astype(jnp.bfloat16)
    gate_act = jnp.dot(normed, gate_sampler, preferred_element_type=jnp.float32)
    up_act = jnp.dot(normed, up_sampler, preferred_element_type=jnp.float32)
    hidden = (jax.nn.silu(gate_act) * up_act).astype(jnp.bfloat16)
    partial_terms = jnp.dot(hidden, down_sampler, preferred_element_type=jnp.float32)
    mixed_out = lax.psum_scatter(partial_terms, "fs", scatter_dimension=1, tiled=True).astype(
        jnp.bfloat16
    )
    return (gate_sampler, up_sampler, down_sampler, mixed_out)


def solution(mesh):
    fs_count, tp_count = mesh.shape["fs"], mesh.shape["tp"]

    def body(tokens, norm_gain, gate_trained, up_trained, down_trained):
        rows, cols = gate_trained.shape
        aligned = (
            tp_count == 4
            and fs_count == 2 * tp_count
            and rows % 256 == 0
            and (cols * tp_count // fs_count) % 128 == 0
            and (down_trained.shape[1] * tp_count // fs_count) % 128 == 0
            and down_trained.shape[0] % 64 == 0
            and tokens.shape[0] % 16 == 0
        )
        run = per_device if aligned else per_device_plain
        return run(tokens, norm_gain, gate_trained, up_trained, down_trained)

    in_specs = (P("tp", None), P("fs"), P("fs", "tp"), P("fs", "tp"), P("fs", "tp"))
    out_specs = (P(None, "fs"), P(None, "fs"), P("fs", None), P("tp", "fs"))
    return jax.shard_map(
        body, mesh=mesh, in_specs=in_specs, out_specs=out_specs, check_vma=False
    )
```

```python
import functools

import jax
import jax.numpy as jnp
from jax import lax
from jax.experimental import pallas as pl
from jax.experimental.pallas import tpu as pltpu
from jax.sharding import PartitionSpec as P

MESH = pl.DeviceIdType.MESH


def handoff_kernel(
    slabs, fs_count, tp_count, chunks,
    gain_ref, tokens_ref, gate_in, up_in, down_in, *refs,
):
    outs, refs = refs[:2], refs[2:]
    down_out, own_out, refs = refs[0], refs[1], refs[2:]
    far_outs, refs = refs[:fs_count - 1], refs[fs_count - 1:]
    (
        land, land_down, own, stage, fbuf, dbuf, normed, act, hidden, own_buf, far_buf, gains,
        fetch_sem, down_sem, token_sem, swap_send, swap_recv, own_send, pass_send, recv,
        core_send, core_recv, cross_send, cross_recv, dx_send, dx_recv, dc_send, dc_recv,
        dp_send, dp_recv, out_sem, down_out_sem, term_sem,
    ) = refs
    ins = (gate_in, up_in)
    blocks, _, rows, owned = own.shape
    down_rows, down_cols = dbuf.shape[1], down_in.shape[1]
    side = fs_count // 2
    cut = rows // 2
    count = len(slabs)
    early = [p for p in range(count) if slabs[p][0] < cut]
    late = [p for p in range(count) if slabs[p][0] >= cut]

    f = lax.axis_index("fs")
    t = lax.axis_index("tp")
    plane, core = lax.div(t, 2), lax.rem(t, 2)
    across = plane * -2 + 2 + core
    partner = plane * 2 + 1 - core
    far_partner = plane * -2 + 3 - core
    z = lax.div(f, blocks)
    half = lax.div(f, side)
    native = half == plane
    foreign = jnp.logical_not(native)
    held_here = lax.rem(z, 2) == core

    def some(condition, body, *args):
        pl.when(condition)(functools.partial(body, *args))

    def remote(src, dst, send, sem, to):
        return pltpu.make_async_remote_copy(
            src_ref=src, dst_ref=dst, send_sem=send, recv_sem=sem, device_id=to,
            device_id_type=MESH,
        )

    def at(m, source, start, size):
        return land.at[m, pl.ds(pl.multiple_of(source * rows + start, 16), size), :]

    def columns(p):
        first = lax.rem(z + p, blocks)
        return [lax.rem(first + k, blocks) for k in range(blocks)]

    def key(p, j, m):
        return p * blocks * 2 + j * 2 + m

    def group(p, within):
        if p in late:
            return p - 1
        return jnp.where(within, 0, p // 2)

    def swap(p, j, m):
        start, size = slabs[p]
        there = pl.ds(start, size)
        return remote(
            own.at[j, m, there, :], stage.at[j, m, there, :],
            swap_send.at[key(0, j, m)], swap_recv.at[key(p, j, m)], (f, across),
        )

    def local_to(target, j, m):
        return jnp.logical_and(target * blocks + j == f, core == m)

    def send_to_owner(held, sems, target, within, p, j, m):
        start, size = slabs[p]
        there = remote(
            held.at[j, m, pl.ds(start, size), :], at(m, f, start, size),
            sems.at[key(0, j, m)], recv.at[f, group(p, within)],
            (target * blocks + j, plane * 2 + m),
        )
        local = local_to(target, j, m)

        @pl.when(local)
        def _():
            @pl.loop(0, size // 16)
            def _(i):
                src = pl.ds(pl.multiple_of(start + i * 16, 16), 16)
                dst = pl.ds(pl.multiple_of(f * rows + start + i * 16, 16), 16)
                land[m, dst, :] = held[j, m, src, :]

        pl.when(jnp.logical_not(local))(there.start)

    def wait_sent(held, sems, target, size, j, m):
        there = held.at[j, m, pl.ds(0, size), :]
        done = remote(there, there, sems.at[key(0, j, m)], recv.at[f, 0], (f, across))
        pl.when(jnp.logical_not(local_to(target, j, m)))(done.wait_send)

    steps = [(p, m) for p in range(count) for m in range(2)]
    depth = fbuf.shape[0]

    def fetch(k):
        p, m = steps[k]
        start, size = slabs[p]
        return pltpu.make_async_copy(
            ins[m].at[pl.ds(start, size), :], fbuf.at[k % depth, pl.ds(0, size), :],
            fetch_sem.at[k % depth],
        )

    def down_fetch(q):
        return pltpu.make_async_copy(
            down_in.at[pl.ds(q * down_rows, down_rows), :], dbuf.at[q % 2], down_sem.at[q % 2]
        )

    def begin(p, m):
        for j in columns(p):
            def crossing(j=j):
                swap(p, j, m).start()

            def direct(j=j):
                send_to_owner(own, own_send, t, native, p, j, m)

            if p == 0:
                direct()
                pl.when(native)(crossing)
            elif p == 1:
                crossing()
                pl.when(native)(direct)
            else:
                crossing()

    for k in range(depth):
        fetch(k).start()
    token_copy = pltpu.make_async_copy(tokens_ref, normed, token_sem)
    token_copy.start()
    barrier = pltpu.get_barrier_semaphore()
    width_of_plane = tp_count // 2
    peers = fs_count * width_of_plane
    place = f * width_of_plane + core

    @pl.loop(1, peers)
    def _(i):
        peer = lax.rem(place + i, peers)
        pl.semaphore_signal(
            barrier, inc=1, device_id_type=MESH,
            device_id=(
                lax.div(peer, width_of_plane),
                plane * width_of_plane + lax.rem(peer, width_of_plane),
            ),
        )

    pl.semaphore_signal(barrier, inc=1, device_id=(f, across), device_id_type=MESH)
    for g in range(rows // 128):
        row = gain_ref[0:1, g * 128:(g + 1) * 128]
        gains[g * 128:(g + 1) * 128, :] = jnp.broadcast_to(row, (128, 128)).T
    for k, (p, m) in enumerate(steps):
        start, size = slabs[p]
        fetch(k).wait()

        @pl.loop(0, size // 16)
        def _(i):
            src = pl.ds(pl.multiple_of(i * 16, 16), 16)
            dst = pl.ds(pl.multiple_of(start + i * 16, 16), 16)
            gain = gains[dst, 0:1]
            for j in range(blocks):
                own[j, m, dst, :] = (
                    gain * fbuf[k % depth, src, j * owned:(j + 1) * owned]
                ).astype(jnp.bfloat16)

        if k + depth < len(steps):
            fetch(k + depth).start()
        if k == 2:
            pl.semaphore_wait(barrier, peers)
            begin(*steps[0])
        if k >= 2:
            begin(*steps[k - 1])
    for q in range(min(2, chunks)):
        down_fetch(q).start()
    begin(*steps[-1])

    def down_at(which, q):
        return land_down.at[
            pl.ds(q * down_rows, down_rows),
            pl.ds(pl.multiple_of(which * down_cols, 128), down_cols),
        ]

    for q in range(chunks):
        down_fetch(q).wait()

        @pl.loop(0, down_rows // 16)
        def _(i):
            src = pl.ds(pl.multiple_of(i * 16, 16), 16)
            dst = pl.ds(pl.multiple_of(q * down_rows + i * 16, 16), 16)
            land_down[dst, pl.ds(pl.multiple_of(t * down_cols, 128), down_cols)] = (
                dbuf[q % 2, src, :].astype(jnp.bfloat16)
            )

        if q + 2 < chunks:
            down_fetch(q + 2).start()

    token_copy.wait()

    @pl.loop(0, normed.shape[0] // 16)
    def _(i):
        dst = pl.ds(pl.multiple_of(i * 16, 16), 16)
        value = normed[dst, :].astype(jnp.float32)
        scale = lax.rsqrt(jnp.mean(value * value, axis=-1, keepdims=True) + 1e-06)
        normed[dst, :] = (value * scale).astype(jnp.bfloat16)
        for m in range(2):
            act[m, dst, :] = jnp.zeros((16, owned), jnp.float32)

    def other(i):
        return (1 - half) * side + lax.rem(f + i, side)

    def same(i):
        return half * side + lax.rem(f + i, side)

    def to_partner(source, p):
        here = at(core, source, *slabs[p])
        return remote(
            here, here, core_send, core_recv.at[source, int(p in late)], (f, partner)
        )

    def wait_partner(source, which):
        here = at(1 - core, source, which * cut, cut)
        remote(here, here, core_send, core_recv.at[source, which], (f, partner)).wait_recv()

    def wait_arrived(source, which, start, size):
        here = at(core, source, start, size)
        remote(here, here, core_send, recv.at[source, which], (f, partner)).wait_recv()

    def crossed(source, p):
        here = at(core, source, *slabs[p])
        return remote(here, here, cross_send, cross_recv.at[source], (f, across))

    def cross_near(p):
        @pl.loop(0, side)
        def _(i):
            source = other(i)
            wait_arrived(source, 0, *slabs[p])
            crossed(source, p).start()
            to_partner(source, p).start()

    def take_far(p):
        @pl.loop(0, side)
        def _(i):
            source = other(i)
            crossed(source, p).wait_recv()
            to_partner(source, p).start()

    def down_cross(q):
        return remote(down_at(t, q), down_at(t, q), dx_send, dx_recv.at[q], (f, across))

    def down_core(which, q):
        return remote(
            down_at(which, q), down_at(which, q), dc_send, dc_recv.at[q], (f, partner)
        )

    def down_pass(which, q):
        return remote(
            down_at(which, q), down_at(which, q), dp_send, dp_recv.at[q], (f, partner)
        )

    def forward(p):
        for j in columns(p):
            for m in range(2):
                swap(p, j, m).wait_recv()
                send_to_owner(stage, pass_send, across, foreign, p, j, m)

    turn = count - 3
    for p in range(count):
        if p == 0:
            pl.when(foreign)(functools.partial(forward, p))
        else:
            forward(p)
        if 2 + p < count:
            for j in columns(2 + p):
                for m in range(2):
                    send_to_owner(own, own_send, t, native, 2 + p, j, m)
        if p == turn:
            some(native, cross_near, 0)
            some(foreign, cross_near, 1)
            for q in range(chunks):
                down_cross(q).start()
                down_core(t, q).start()

    def take(source, p, which):
        wait_arrived(source, which, *slabs[p])
        to_partner(source, p).start()

    def take_within(source, ps, which):
        @pl.when(jnp.logical_not(jnp.logical_and(source == f, held_here)))
        def _():
            start = slabs[ps[0]][0]
            wait_arrived(source, which, start, sum(slabs[p][1] for p in ps))

        for p in ps:
            to_partner(source, p).start()

    def multiply(source, lo, size):
        lanes = pl.ds(pl.multiple_of(source * rows + lo, 128), size)
        left = normed[:, lanes]
        for m in range(2):
            act[m] += jnp.dot(
                left, land[m, pl.ds(pl.multiple_of(source * rows + lo, 16), size), :],
                preferred_element_type=jnp.float32,
            )

    def out_copy(source, m):
        here = pl.ds(pl.multiple_of(source * rows, 16), rows)
        return pltpu.make_async_copy(land.at[m, here, :], outs[m].at[here, :], out_sem.at[m])

    @pl.loop(0, side)
    def _(i):
        take_within(same(i), early, 0)

    @pl.loop(0, side)
    def _(i):
        take(other(i), 2, 1)

    some(native, take_far, 1)
    some(foreign, take_far, 0)

    @pl.loop(0, fs_count)
    def _(i):
        source = lax.rem(half * side + i, fs_count)
        wait_partner(source, 0)
        multiply(source, 0, cut)

    def down_on(q):
        down_in_here = remote(
            down_at(across, q), down_at(across, q), dx_send, dx_recv.at[q], (f, across)
        )
        down_in_here.wait_recv()
        down_pass(across, q).start()

    def down_done(q):
        down_core(partner, q).wait_recv()
        down_pass(far_partner, q).wait_recv()
        here = pl.ds(q * down_rows, down_rows)
        return pltpu.make_async_copy(
            land_down.at[here, :], down_out.at[here, :], down_out_sem
        )

    for n, p in enumerate(late[:-1]):
        @pl.loop(0, side)
        def _(i):
            take_within(same(i), [p], p - 1)

        @pl.loop(0, side)
        def _(i):
            take(other(i), p, p - 1)

        if n < chunks - 2:
            down_on(n)
        if 0 < n < chunks - 2:
            down_done(n - 1).start()
    last_p = late[-1]

    def finish(source):
        wait_partner(source, 1)
        multiply(source, cut, rows - cut)
        for m in range(2):
            out_copy(source, m).start()

    @pl.loop(0, side)
    def _(i):
        take_within(same(i), [last_p], last_p - 1)

    @pl.loop(0, side)
    def _(i):
        finish(same(i))

    for q in range(len(late) - 1, chunks - 1):
        down_on(q)
        down_done(q - 1).start()

    @pl.loop(0, side)
    def _(i):
        take(other(i), last_p, last_p - 1)

        @pl.when(i > 0)
        def _():
            finish(other(i - 1))

    for q in range(max(0, chunks - 1), chunks):
        down_on(q)
    finish(other(side - 1))
    down_done(chunks - 2).start()

    @pl.loop(0, normed.shape[0] // 16)
    def _(i):
        dst = pl.ds(pl.multiple_of(i * 16, 16), 16)
        gate = act[0, dst, :]
        small = jnp.exp(-jnp.abs(gate))
        silu = gate * jnp.where(gate >= 0, 1.0, small) / (1.0 + small)
        hidden[dst, :] = (silu * act[1, dst, :]).astype(jnp.bfloat16)

    down_done(chunks - 1).start()
    width = own_buf.shape[1]

    def term(b):
        lanes = pl.ds(pl.multiple_of(b * width, 128), width)
        return jnp.dot(hidden[...], land_down[:, lanes], preferred_element_type=jnp.float32)

    def put_term(k):
        if k == 0:
            return pltpu.make_async_copy(own_buf, own_out, term_sem.at[0])
        return pltpu.make_async_copy(far_buf.at[k - 1], far_outs[k - 1], term_sem.at[k])

    for k in range(1, fs_count):
        far_buf[k - 1] = term(lax.rem(f + k, fs_count)).astype(jnp.bfloat16)
        if k > 1:
            put_term(k - 1).start()
    own_buf[...] = term(f)
    put_term(fs_count - 1).start()

    def wait_kept(crossing, direct, passed):
        for j in range(blocks):
            for m in range(2):
                there = own.at[j, m, pl.ds(0, crossing), :]
                remote(
                    there, there, swap_send.at[key(0, j, m)], swap_recv.at[0], (f, across)
                ).wait_send()
                wait_sent(own, own_send, t, direct, j, m)
                wait_sent(stage, pass_send, across, passed, j, m)

    def wait_crossed(p):
        here = land.at[0, pl.ds(0, side * slabs[p][1]), :]
        remote(here, here, cross_send, cross_recv.at[0], (f, across)).wait_send()

    first, second = slabs[0][1], slabs[1][1]
    some(native, wait_kept, rows, rows, rows - first)
    some(foreign, wait_kept, rows - first, rows - second, rows)
    put_term(0).start()
    some(native, wait_crossed, 0)
    some(foreign, wait_crossed, 1)
    remote(land.at[core], land.at[core], core_send, recv.at[0, 0], (f, partner)).wait_send()
    for m in range(2):
        pltpu.make_async_copy(land.at[m], outs[m], out_sem.at[m]).wait()
    whole = land_down.at[:, pl.ds(0, down_cols)]
    for sem in (dx_send, dc_send, dp_send):
        remote(whole, whole, sem, dx_recv.at[0], (f, partner)).wait_send()
    pltpu.make_async_copy(land_down, down_out, down_out_sem).wait()
    for k in range(fs_count):
        put_term(k).wait()


def row_slabs(rows):
    first = max(16, (rows * 7 // 32) // 16 * 16)
    second = max(16, (rows * 6 // 32) // 16 * 16)
    cut = rows // 2
    slabs = [(0, first), (first, second), (first + second, cut - first - second)]
    left, start = (rows - cut) // 16, cut
    for k in range(3):
        size = -(-left // (3 - k)) * 16
        slabs.append((start, size))
        start, left = start + size, left - size // 16
    return slabs


def handoff(fs_count, tp_count, chunks, tokens, norm_gain, gate, up, down):
    rows, cols = gate.shape
    blocks = fs_count // tp_count
    owned = cols // blocks
    width = down.shape[1] * tp_count // fs_count
    down_rows, down_cols = down.shape
    model = rows * fs_count
    count = tokens.shape[0]
    slabs = row_slabs(rows)
    parts = len(slabs)
    f32, bf16, dma = jnp.float32, jnp.bfloat16, pltpu.SemaphoreType.DMA
    anywhere = pl.BlockSpec(memory_space=pl.ANY)
    tall = max(size for _, size in slabs)
    pieces = parts * blocks * 2
    return pl.pallas_call(
        functools.partial(handoff_kernel, slabs, fs_count, tp_count, chunks),
        out_shape=[
            jax.ShapeDtypeStruct((model, owned), bf16),
            jax.ShapeDtypeStruct((model, owned), bf16),
            jax.ShapeDtypeStruct((down_rows, down_cols * tp_count), bf16),
            jax.ShapeDtypeStruct((count, width), f32),
        ] + [jax.ShapeDtypeStruct((count, width), bf16)] * (fs_count - 1),
        in_specs=[pl.BlockSpec(memory_space=pltpu.VMEM)] + [anywhere] * 4,
        out_specs=[anywhere] * (3 + fs_count),
        scratch_shapes=[
            pltpu.VMEM((2, model, owned), bf16),
            pltpu.VMEM((down_rows, down_cols * tp_count), bf16),
            pltpu.VMEM((blocks, 2, rows, owned), bf16),
            pltpu.VMEM((blocks, 2, rows, owned), bf16),
            pltpu.VMEM((3, tall, cols), f32),
            pltpu.VMEM((2, down_rows // chunks, down_cols), f32),
            pltpu.VMEM(tokens.shape, bf16),
            pltpu.VMEM((2, count, owned), f32),
            pltpu.VMEM((count, owned), bf16),
            pltpu.VMEM((count, width), f32),
            pltpu.VMEM((fs_count - 1, count, width), bf16),
            pltpu.VMEM((rows, 128), f32),
            dma((3,)), dma((2,)), dma(()),
            dma((blocks * 2,)), dma((pieces,)), dma((blocks * 2,)), dma((blocks * 2,)),
            dma((fs_count, parts - 1)), dma(()), dma((fs_count, 2)),
            dma(()), dma((fs_count,)),
            dma(()), dma((chunks,)), dma(()), dma((chunks,)), dma(()), dma((chunks,)),
            dma((2,)), dma(()), dma((fs_count,)),
        ],
        compiler_params=pltpu.CompilerParams(
            collective_id=0, has_side_effects=True, vmem_limit_bytes=62 * 1024 * 1024
        ),
    )(norm_gain[None, :], tokens, gate, up, down)


def put_out(landed):
    slots = 16

    def cut(array):
        target = max(16, (720 * 1024) // (array.shape[1] * array.dtype.itemsize))
        return max(r for r in range(16, array.shape[0] + 1, 16) if array.shape[0] % r == 0 and r <= target)

    sizes = [cut(a) for a in landed]
    blocks = [(n, k * size) for n, size in enumerate(sizes) for k in range(landed[n].shape[0] // size)]
    count = len(landed)

    def copy_kernel(*refs):
        ins, outs, bufs = refs[:count], refs[count:2 * count], refs[2 * count:3 * count]
        read_sem, write_sem = refs[3 * count:]

        def read(k):
            n, start = blocks[k]
            return pltpu.make_async_copy(
                ins[n].at[pl.ds(start, sizes[n]), :], bufs[n].at[k % slots], read_sem.at[k % slots]
            )

        def write(k):
            n, start = blocks[k]
            return pltpu.make_async_copy(
                bufs[n].at[k % slots], outs[n].at[pl.ds(start, sizes[n]), :], write_sem.at[k % slots]
            )

        ahead = slots // 2
        for k in range(min(ahead, len(blocks))):
            read(k).start()
        for k in range(len(blocks)):
            read(k).wait()
            write(k).start()
            if k + ahead < len(blocks):
                if k + ahead >= slots:
                    write(k + ahead - slots).wait()
                read(k + ahead).start()
        for k in range(max(0, len(blocks) - slots), len(blocks)):
            write(k).wait()

    anywhere = pl.BlockSpec(memory_space=pl.ANY)
    return pl.pallas_call(
        copy_kernel,
        out_shape=[jax.ShapeDtypeStruct(a.shape, a.dtype) for a in landed],
        in_specs=[anywhere] * count,
        out_specs=[anywhere] * count,
        scratch_shapes=[
            pltpu.VMEM((slots, size, a.shape[1]), a.dtype) for a, size in zip(landed, sizes)
        ] + [pltpu.SemaphoreType.DMA((slots,)), pltpu.SemaphoreType.DMA((slots,))],
        compiler_params=pltpu.CompilerParams(vmem_limit_bytes=48 * 1024 * 1024),
        cost_estimate=pl.CostEstimate(
            flops=0, bytes_accessed=4 * sum(a.size for a in landed), transcendentals=0
        ),
    )(*landed)


def scatter_sum(own, far, fs_count):
    arrived = []
    for k in range(1, fs_count):
        ring = [(i, (i + k) % fs_count) for i in range(fs_count)]
        arrived.append(lax.ppermute(far[k - 1], "fs", ring))
    total = own
    for piece in arrived:
        total = total + piece.astype(jnp.float32)
    return total.astype(jnp.bfloat16)


def per_device(tokens, norm_gain, gate_trained, up_trained, down_trained):
    tp_count = lax.axis_size("tp")
    fs_count = lax.axis_size("fs")
    gate_sampler, up_sampler, down_sampler, own, *far = handoff(
        fs_count, tp_count, 4, tokens, norm_gain, gate_trained, up_trained, down_trained
    )
    mixed = scatter_sum(own, far, fs_count)
    return (*put_out((gate_sampler, up_sampler, down_sampler)), mixed)


def per_device_plain(tokens, norm_gain, gate_trained, up_trained, down_trained):
    gate_local = (norm_gain[:, None] * gate_trained).astype(jnp.bfloat16)
    up_local = (norm_gain[:, None] * up_trained).astype(jnp.bfloat16)
    down_local = down_trained.astype(jnp.bfloat16)
    tp_count = lax.axis_size("tp")
    fs_count = lax.axis_size("fs")
    rows_local = gate_local.shape[0]
    cols_local = gate_local.shape[1]
    model_width = rows_local * fs_count
    owned_count = cols_local * tp_count // fs_count
    piece_cols = owned_count // tp_count
    block_count = cols_local // owned_count

    def arrange(matrix):
        return matrix.reshape(rows_local, block_count, tp_count, piece_cols)

    gate_mixed, up_mixed = (
        lax.all_to_all(arrange(gate_local), "tp", split_axis=2, concat_axis=2, tiled=True),
        lax.all_to_all(arrange(up_local), "tp", split_axis=2, concat_axis=2, tiled=True),
    )

    def regroup(matrix):
        return matrix.transpose(2, 1, 0, 3).reshape(fs_count, rows_local, piece_cols)

    gate_parts, up_parts = (
        lax.all_to_all(regroup(gate_mixed), "fs", split_axis=0, concat_axis=1, tiled=True),
        lax.all_to_all(regroup(up_mixed), "fs", split_axis=0, concat_axis=1, tiled=True),
    )
    gate_sampler, up_sampler, down_sampler = (
        lax.all_gather(gate_parts.reshape(model_width, piece_cols), "tp", axis=1, tiled=True),
        lax.all_gather(up_parts.reshape(model_width, piece_cols), "tp", axis=1, tiled=True),
        lax.all_gather(down_local, "tp", axis=1, tiled=True),
    )
    as_float = tokens.astype(jnp.float32)
    normed = (
        as_float * lax.rsqrt(jnp.mean(as_float * as_float, axis=-1, keepdims=True) + 1e-06)
    ).astype(jnp.bfloat16)
    gate_act = jnp.dot(normed, gate_sampler, preferred_element_type=jnp.float32)
    up_act = jnp.dot(normed, up_sampler, preferred_element_type=jnp.float32)
    hidden = (jax.nn.silu(gate_act) * up_act).astype(jnp.bfloat16)
    partial_terms = jnp.dot(hidden, down_sampler, preferred_element_type=jnp.float32)
    mixed_out = lax.psum_scatter(partial_terms, "fs", scatter_dimension=1, tiled=True).astype(
        jnp.bfloat16
    )
    return (gate_sampler, up_sampler, down_sampler, mixed_out)


def solution(mesh):
    fs_count, tp_count = mesh.shape["fs"], mesh.shape["tp"]

    def body(tokens, norm_gain, gate_trained, up_trained, down_trained):
        rows, cols = gate_trained.shape
        aligned = (
            tp_count == 4
            and fs_count == 2 * tp_count
            and rows % 256 == 0
            and (cols * tp_count // fs_count) % 128 == 0
            and (down_trained.shape[1] * tp_count // fs_count) % 128 == 0
            and down_trained.shape[0] % 64 == 0
            and tokens.shape[0] % 16 == 0
        )
        run = per_device if aligned else per_device_plain
        return run(tokens, norm_gain, gate_trained, up_trained, down_trained)

    in_specs = (P("tp", None), P("fs"), P("fs", "tp"), P("fs", "tp"), P("fs", "tp"))
    out_specs = (P(None, "fs"), P(None, "fs"), P("fs", None), P("tp", "fs"))
    return jax.shard_map(
        body, mesh=mesh, in_specs=in_specs, out_specs=out_specs, check_vma=False
    )
```

```python
import functools

import jax
import jax.numpy as jnp
from jax import lax
from jax.experimental import pallas as pl
from jax.experimental.pallas import tpu as pltpu
from jax.sharding import PartitionSpec as P

MESH = pl.DeviceIdType.MESH


def sent_terms(fs_count):
    half = fs_count // 2
    return [k for k in [*range(half, fs_count), *range(1, half)] if k not in paired(fs_count)]


def paired(fs_count):
    return [fs_count - 1 - 2 * i for i in range(2)]


def handoff_kernel(
    slabs, fs_count, tp_count, chunks,
    gain_ref, tokens_ref, gate_in, up_in, down_in, *refs,
):
    land, land_down, own_out, refs = refs[0], refs[1], refs[2], refs[3:]
    sent, pairs = sent_terms(fs_count), paired(fs_count)
    far_outs, refs = refs[:len(sent)], refs[len(sent):]
    (
        own, stage, fbuf, dbuf, normed, act, hidden, own_buf, far_buf, gains,
        pair_buf, pair_in, pair_send, pair_recv,
        fetch_sem, down_sem, token_sem, swap_send, swap_recv, own_send, pass_send, recv,
        core_send, core_recv, cross_send, cross_recv, dx_send, dx_recv, dc_send, dc_recv,
        dp_send, dp_recv, term_sem,
    ) = refs
    ins = (gate_in, up_in)
    blocks, _, rows, owned = own.shape
    down_rows, down_cols = dbuf.shape[1], down_in.shape[1]
    side = fs_count // 2
    cut = rows // 2
    count = len(slabs)
    early = [p for p in range(count) if slabs[p][0] < cut]
    late = [p for p in range(count) if slabs[p][0] >= cut]

    f = lax.axis_index("fs")
    t = lax.axis_index("tp")
    plane, core = lax.div(t, 2), lax.rem(t, 2)
    across = plane * -2 + 2 + core
    partner = plane * 2 + 1 - core
    far_partner = plane * -2 + 3 - core
    z = lax.div(f, blocks)
    half = lax.div(f, side)
    native = half == plane
    foreign = jnp.logical_not(native)
    held_here = lax.rem(z, 2) == core

    def some(condition, body, *args):
        pl.when(condition)(functools.partial(body, *args))

    def remote(src, dst, send, sem, to):
        return pltpu.make_async_remote_copy(
            src_ref=src, dst_ref=dst, send_sem=send, recv_sem=sem, device_id=to,
            device_id_type=MESH,
        )

    def at(m, source, start, size):
        return land.at[m, pl.ds(pl.multiple_of(source * rows + start, 16), size), :]

    def columns(p):
        first = lax.rem(z + p, blocks)
        return [lax.rem(first + k, blocks) for k in range(blocks)]

    def key(p, j, m):
        return p * blocks * 2 + j * 2 + m

    def group(p, within):
        if p in late:
            return p - 1
        return jnp.where(within, 0, p // 2)

    def cuts(p):
        start, size = slabs[p]
        if p != 1 or size <= 32:
            return [(start, size)]
        return [(start, 32), (start + 32, size - 32)]

    def swap(p, j, m, n=0):
        there = pl.ds(*cuts(p)[n])
        return remote(
            own.at[j, m, there, :], stage.at[j, m, there, :],
            swap_send.at[key(0, j, m)], swap_recv.at[key(count if n else p, j, m)], (f, across),
        )

    def local_to(target, j, m):
        return jnp.logical_and(target * blocks + j == f, core == m)

    def send_to_owner(held, sems, target, within, p, j, m, piece=None):
        start, size = piece or slabs[p]
        there = remote(
            held.at[j, m, pl.ds(start, size), :], at(m, f, start, size),
            sems.at[key(0, j, m)], recv.at[f, group(p, within)],
            (target * blocks + j, plane * 2 + m),
        )
        local = local_to(target, j, m)

        @pl.when(local)
        def _():
            @pl.loop(0, size // 16)
            def _(i):
                src = pl.ds(pl.multiple_of(start + i * 16, 16), 16)
                dst = pl.ds(pl.multiple_of(f * rows + start + i * 16, 16), 16)
                land[m, dst, :] = held[j, m, src, :]

        pl.when(jnp.logical_not(local))(there.start)

    def wait_sent(held, sems, target, size, j, m):
        there = held.at[j, m, pl.ds(0, size), :]
        done = remote(there, there, sems.at[key(0, j, m)], recv.at[f, 0], (f, across))
        pl.when(jnp.logical_not(local_to(target, j, m)))(done.wait_send)

    steps = [(p, m) for p in range(count) for m in range(2)]
    depth = fbuf.shape[0]

    def fetch(k):
        p, m = steps[k]
        start, size = slabs[p]
        return pltpu.make_async_copy(
            ins[m].at[pl.ds(start, size), :], fbuf.at[k % depth, pl.ds(0, size), :],
            fetch_sem.at[k % depth],
        )

    def down_fetch(q):
        return pltpu.make_async_copy(
            down_in.at[pl.ds(q * down_rows, down_rows), :], dbuf.at[q % 2], down_sem.at[q % 2]
        )

    def begin(p, m):
        for j in columns(p):
            def crossing(j=j):
                swap(p, j, m).start()

            if len(cuts(p)) > 1:
                continue

            def direct(j=j):
                send_to_owner(own, own_send, t, native, p, j, m)

            if p == 0:
                direct()
                pl.when(native)(crossing)
            elif p == 1:
                crossing()
                pl.when(native)(direct)
            else:
                crossing()

        if len(cuts(p)) > 1:
            for n in range(2):
                for j in columns(p):
                    swap(p, j, m, n).start()

            @pl.when(native)
            def _():
                for j in columns(p):
                    send_to_owner(own, own_send, t, native, p, j, m)

    for k in range(depth):
        fetch(k).start()
    token_copy = pltpu.make_async_copy(tokens_ref, normed, token_sem)
    token_copy.start()
    barrier = pltpu.get_barrier_semaphore()
    width_of_plane = tp_count // 2
    peers = fs_count * width_of_plane
    place = f * width_of_plane + core

    @pl.loop(1, peers)
    def _(i):
        peer = lax.rem(place + i, peers)
        pl.semaphore_signal(
            barrier, inc=1, device_id_type=MESH,
            device_id=(
                lax.div(peer, width_of_plane),
                plane * width_of_plane + lax.rem(peer, width_of_plane),
            ),
        )

    pl.semaphore_signal(barrier, inc=1, device_id=(f, across), device_id_type=MESH)
    for g in range(rows // 128):
        row = gain_ref[0:1, g * 128:(g + 1) * 128]
        gains[g * 128:(g + 1) * 128, :] = jnp.broadcast_to(row, (128, 128)).T
    for k, (p, m) in enumerate(steps):
        start, size = slabs[p]
        fetch(k).wait()

        @pl.loop(0, size // 16)
        def _(i):
            src = pl.ds(pl.multiple_of(i * 16, 16), 16)
            dst = pl.ds(pl.multiple_of(start + i * 16, 16), 16)
            gain = gains[dst, 0:1]
            for j in range(blocks):
                own[j, m, dst, :] = (
                    gain * fbuf[k % depth, src, j * owned:(j + 1) * owned]
                ).astype(jnp.bfloat16)

        if k + depth < len(steps):
            fetch(k + depth).start()
        if k == 2:
            pl.semaphore_wait(barrier, peers)
            begin(*steps[0])
        if k >= 2:
            begin(*steps[k - 1])
    for q in range(min(2, chunks)):
        down_fetch(q).start()
    begin(*steps[-1])

    def down_at(which, q):
        return land_down.at[
            pl.ds(q * down_rows, down_rows),
            pl.ds(pl.multiple_of(which * down_cols, 128), down_cols),
        ]

    for q in range(chunks):
        down_fetch(q).wait()

        @pl.loop(0, down_rows // 16)
        def _(i):
            src = pl.ds(pl.multiple_of(i * 16, 16), 16)
            dst = pl.ds(pl.multiple_of(q * down_rows + i * 16, 16), 16)
            land_down[dst, pl.ds(pl.multiple_of(t * down_cols, 128), down_cols)] = (
                dbuf[q % 2, src, :].astype(jnp.bfloat16)
            )

        if q + 2 < chunks:
            down_fetch(q + 2).start()

    token_copy.wait()

    @pl.loop(0, normed.shape[0] // 16)
    def _(i):
        dst = pl.ds(pl.multiple_of(i * 16, 16), 16)
        value = normed[dst, :].astype(jnp.float32)
        scale = lax.rsqrt(jnp.mean(value * value, axis=-1, keepdims=True) + 1e-06)
        normed[dst, :] = (value * scale).astype(jnp.bfloat16)
        for m in range(2):
            act[m, dst, :] = jnp.zeros((16, owned), jnp.float32)

    def other(i):
        return (1 - half) * side + lax.rem(f + i, side)

    def same(i):
        return half * side + lax.rem(f + i, side)

    def to_partner(source, p):
        here = at(core, source, *slabs[p])
        return remote(
            here, here, core_send, core_recv.at[source, int(p in late)], (f, partner)
        )

    def wait_partner(source, which):
        here = at(1 - core, source, which * cut, cut)
        remote(here, here, core_send, core_recv.at[source, which], (f, partner)).wait_recv()

    def wait_arrived(source, which, start, size):
        here = at(core, source, start, size)
        remote(here, here, core_send, recv.at[source, which], (f, partner)).wait_recv()

    def crossed(source, p):
        here = at(core, source, *slabs[p])
        return remote(here, here, cross_send, cross_recv.at[source], (f, across))

    def cross_near(p):
        @pl.loop(0, side)
        def _(i):
            source = other(i)
            wait_arrived(source, 0, *slabs[p])
            crossed(source, p).start()
            to_partner(source, p).start()

    def take_far(p):
        @pl.loop(0, side)
        def _(i):
            source = other(i)
            crossed(source, p).wait_recv()
            to_partner(source, p).start()

    def down_cross(q):
        return remote(down_at(t, q), down_at(t, q), dx_send, dx_recv.at[q], (f, across))

    def down_core(which, q):
        return remote(
            down_at(which, q), down_at(which, q), dc_send, dc_recv.at[q], (f, partner)
        )

    def down_pass(which, q):
        return remote(
            down_at(which, q), down_at(which, q), dp_send, dp_recv.at[q], (f, partner)
        )

    def forward(p):
        for m in range(2):
            for n, piece in enumerate(cuts(p)):
                for j in columns(p):
                    swap(p, j, m, n).wait_recv()
                    send_to_owner(stage, pass_send, across, foreign, p, j, m, piece)

    turn = count - 3
    for p in range(count):
        if p == 0:
            pl.when(foreign)(functools.partial(forward, p))
        else:
            forward(p)
        if 2 + p < count:
            for j in columns(2 + p):
                for m in range(2):
                    send_to_owner(own, own_send, t, native, 2 + p, j, m)
        if p == turn:
            some(native, cross_near, 0)
            some(foreign, cross_near, 1)
            for q in range(chunks):
                down_cross(q).start()
                down_core(t, q).start()

    def take(source, p, which):
        wait_arrived(source, which, *slabs[p])
        to_partner(source, p).start()

    def take_within(source, ps, which):
        @pl.when(jnp.logical_not(jnp.logical_and(source == f, held_here)))
        def _():
            start = slabs[ps[0]][0]
            wait_arrived(source, which, start, sum(slabs[p][1] for p in ps))

        for p in ps:
            to_partner(source, p).start()

    def multiply(source, lo, size):
        lanes = pl.ds(pl.multiple_of(source * rows + lo, 128), size)
        left = normed[:, lanes]
        for m in range(2):
            act[m] += jnp.dot(
                left, land[m, pl.ds(pl.multiple_of(source * rows + lo, 16), size), :],
                preferred_element_type=jnp.float32,
            )

    @pl.loop(0, side)
    def _(i):
        take_within(same(i), early, 0)

    @pl.loop(0, side)
    def _(i):
        take(other(i), 2, 1)

    some(native, take_far, 1)
    some(foreign, take_far, 0)

    @pl.loop(0, fs_count)
    def _(i):
        source = lax.rem(half * side + i, fs_count)
        wait_partner(source, 0)
        multiply(source, 0, cut)

    def down_on(q):
        down_in_here = remote(
            down_at(across, q), down_at(across, q), dx_send, dx_recv.at[q], (f, across)
        )
        down_in_here.wait_recv()
        down_pass(across, q).start()

    def down_done(q):
        down_core(partner, q).wait_recv()
        down_pass(far_partner, q).wait_recv()

    for n, p in enumerate(late[:-1]):
        @pl.loop(0, side)
        def _(i):
            take_within(same(i), [p], p - 1)

        @pl.loop(0, side)
        def _(i):
            take(other(i), p, p - 1)

        if n < chunks - 2:
            down_on(n)
        if 0 < n < chunks - 2:
            down_done(n - 1)
    last_p = late[-1]

    def finish(source):
        wait_partner(source, 1)
        multiply(source, cut, rows - cut)

    @pl.loop(0, side)
    def _(i):
        take_within(same(i), [last_p], last_p - 1)

    @pl.loop(0, side)
    def _(i):
        finish(same(i))

    for q in range(len(late) - 1, chunks - 1):
        down_on(q)
        down_done(q - 1)

    @pl.loop(0, side)
    def _(i):
        take(other(i), last_p, last_p - 1)

        @pl.when(i > 0)
        def _():
            finish(other(i - 1))

    for q in range(max(0, chunks - 1), chunks):
        down_on(q)
    finish(other(side - 1))
    down_done(chunks - 2)

    @pl.loop(0, normed.shape[0] // 16)
    def _(i):
        dst = pl.ds(pl.multiple_of(i * 16, 16), 16)
        gate = act[0, dst, :]
        small = jnp.exp(-jnp.abs(gate))
        silu = gate * jnp.where(gate >= 0, 1.0, small) / (1.0 + small)
        hidden[dst, :] = (silu * act[1, dst, :]).astype(jnp.bfloat16)

    down_done(chunks - 1)
    width = own_buf.shape[1]

    def peer(k):
        return sum(lax.rem(lax.div(f, n) + k // n, 2) * n for n in (1, 2, 4))

    def term(b):
        lanes = pl.ds(pl.multiple_of(b * width, 128), width)
        return jnp.dot(hidden[...], land_down[:, lanes], preferred_element_type=jnp.float32)

    def put_term(k):
        if k == 0:
            return pltpu.make_async_copy(own_buf, own_out, term_sem.at[0])
        return pltpu.make_async_copy(far_buf.at[k - 1], far_outs[sent.index(k)], term_sem.at[k])

    def to_pair(i):
        return remote(
            far_buf.at[pairs[i] - 1], pair_in.at[i], pair_send.at[i], pair_recv.at[i], (peer(1), t)
        )

    for i, k in enumerate(pairs):
        far_buf[k - 1] = term(peer(k)).astype(jnp.bfloat16)
        if i:
            to_pair(i - 1).start()
    summed = [k - 1 for k in pairs]
    for i, k in enumerate(summed):
        pair_buf[i] = term(peer(k))
        if i == 0:
            to_pair(len(pairs) - 1).start()
    held_back = None
    for k in sent:
        if k in summed:
            continue
        far_buf[k - 1] = term(peer(k)).astype(jnp.bfloat16)
        if held_back:
            put_term(held_back).start()
        held_back = k
    own_buf[...] = term(f)
    put_term(held_back).start()
    for i, k in enumerate(summed):
        to_pair(i).wait_recv()
        far_buf[k - 1] = (pair_buf[i] + pair_in[i].astype(jnp.float32)).astype(jnp.bfloat16)
        put_term(0 if i == 0 else summed[i - 1]).start()

    def wait_kept(crossing, direct, passed):
        for j in range(blocks):
            for m in range(2):
                there = own.at[j, m, pl.ds(0, crossing), :]
                remote(
                    there, there, swap_send.at[key(0, j, m)], swap_recv.at[0], (f, across)
                ).wait_send()
                wait_sent(own, own_send, t, direct, j, m)
                wait_sent(stage, pass_send, across, passed, j, m)

    def wait_crossed(p):
        here = land.at[0, pl.ds(0, side * slabs[p][1]), :]
        remote(here, here, cross_send, cross_recv.at[0], (f, across)).wait_send()

    first, second = slabs[0][1], slabs[1][1]
    some(native, wait_kept, rows, rows, rows - first)
    some(foreign, wait_kept, rows - first, rows - second, rows)
    put_term(summed[-1]).start()
    some(native, wait_crossed, 0)
    some(foreign, wait_crossed, 1)
    remote(land.at[core], land.at[core], core_send, recv.at[0, 0], (f, partner)).wait_send()
    whole = land_down.at[:, pl.ds(0, down_cols)]
    for sem in (dx_send, dc_send, dp_send):
        remote(whole, whole, sem, dx_recv.at[0], (f, partner)).wait_send()
    for i in range(len(pairs)):
        to_pair(i).wait_send()
    for k in [0, *sent]:
        put_term(k).wait()


def row_slabs(rows):
    first = max(16, (rows * 6 // 32) // 16 * 16)
    second = max(16, (rows * 6 // 32) // 16 * 16)
    cut = rows // 2
    slabs = [(0, first), (first, second), (first + second, cut - first - second)]
    left, start = (rows - cut) // 16, cut
    for k in range(3):
        size = -(-left // (3 - k)) * 16
        slabs.append((start, size))
        start, left = start + size, left - size // 16
    return slabs


def handoff(fs_count, tp_count, chunks, tokens, norm_gain, gate, up, down):
    rows, cols = gate.shape
    blocks = fs_count // tp_count
    owned = cols // blocks
    width = down.shape[1] * tp_count // fs_count
    down_rows, down_cols = down.shape
    model = rows * fs_count
    count = tokens.shape[0]
    slabs = row_slabs(rows)
    parts = len(slabs)
    f32, bf16, dma = jnp.float32, jnp.bfloat16, pltpu.SemaphoreType.DMA
    anywhere = pl.BlockSpec(memory_space=pl.ANY)
    inside = pl.BlockSpec(memory_space=pltpu.VMEM)
    tall = max(size for _, size in slabs)
    pieces = (parts + 1) * blocks * 2
    pairs = len(paired(fs_count))
    return pl.pallas_call(
        functools.partial(handoff_kernel, slabs, fs_count, tp_count, chunks),
        out_shape=[
            pltpu.VMEM((2, model, owned), bf16),
            pltpu.VMEM((down_rows, down_cols * tp_count), bf16),
            jax.ShapeDtypeStruct((count, width), f32),
        ] + [jax.ShapeDtypeStruct((count, width), bf16)] * len(sent_terms(fs_count)),
        in_specs=[inside] + [anywhere] * 4,
        out_specs=[inside] * 2 + [anywhere] * (1 + len(sent_terms(fs_count))),
        scratch_shapes=[
            pltpu.VMEM((blocks, 2, rows, owned), bf16),
            pltpu.VMEM((blocks, 2, rows, owned), bf16),
            pltpu.VMEM((3, tall, cols), f32),
            pltpu.VMEM((2, down_rows // chunks, down_cols), f32),
            pltpu.VMEM(tokens.shape, bf16),
            pltpu.VMEM((2, count, owned), f32),
            pltpu.VMEM((count, owned), bf16),
            pltpu.VMEM((count, width), f32),
            pltpu.VMEM((fs_count - 1, count, width), bf16),
            pltpu.VMEM((rows, 128), f32),
            pltpu.VMEM((pairs, count, width), f32), pltpu.VMEM((pairs, count, width), bf16),
            dma((pairs,)), dma((pairs,)),
            dma((3,)), dma((2,)), dma(()),
            dma((blocks * 2,)), dma((pieces,)), dma((blocks * 2,)), dma((blocks * 2,)),
            dma((fs_count, parts - 1)), dma(()), dma((fs_count, 2)),
            dma(()), dma((fs_count,)),
            dma(()), dma((chunks,)), dma(()), dma((chunks,)), dma(()), dma((chunks,)),
            dma((fs_count,)),
        ],
        compiler_params=pltpu.CompilerParams(
            collective_id=0, has_side_effects=True, vmem_limit_bytes=29 * 1024 * 1024
        ),
    )(norm_gain[None, :], tokens, gate, up, down)


def put_out(land, land_down):
    def copy_kernel(land_ref, down_ref, gate_ref, up_ref, down_out_ref, sems):
        copies = []
        for source, target in ((land_ref.at[0], gate_ref), (land_ref.at[1], up_ref), (down_ref, down_out_ref)):
            tall = target.shape[0] // 8
            for k in range(8):
                here = pl.ds(k * tall, tall)
                copies.append(pltpu.make_async_copy(source.at[here, :], target.at[here, :], sems.at[len(copies)]))
        for c in copies:
            c.start()
        for c in copies:
            c.wait()

    anywhere = pl.BlockSpec(memory_space=pl.ANY)
    inside = pl.BlockSpec(memory_space=pltpu.VMEM)
    return pl.pallas_call(
        copy_kernel,
        out_shape=[
            jax.ShapeDtypeStruct(land.shape[1:], land.dtype),
            jax.ShapeDtypeStruct(land.shape[1:], land.dtype),
            jax.ShapeDtypeStruct(land_down.shape, land_down.dtype),
        ],
        in_specs=[inside] * 2,
        out_specs=[anywhere] * 3,
        scratch_shapes=[pltpu.SemaphoreType.DMA((24,))],
        compiler_params=pltpu.CompilerParams(vmem_limit_bytes=29 * 1024 * 1024),
        cost_estimate=pl.CostEstimate(
            flops=0, bytes_accessed=4 * (land.size + land_down.size), transcendentals=0
        ),
    )(pltpu.with_memory_space_constraint(land, pltpu.VMEM), pltpu.with_memory_space_constraint(land_down, pltpu.VMEM))


def scatter_sum(own, far, fs_count):
    arrived = []
    for k, sent in zip(sent_terms(fs_count), far):
        ring = [(i, i ^ k) for i in range(fs_count)]
        arrived.append(lax.ppermute(sent, "fs", ring))
    total = own
    for piece in arrived:
        total = total + piece.astype(jnp.float32)
    return total.astype(jnp.bfloat16)


def per_device(tokens, norm_gain, gate_trained, up_trained, down_trained):
    tp_count = lax.axis_size("tp")
    fs_count = lax.axis_size("fs")
    land, land_down, own, *far = handoff(
        fs_count, tp_count, 4, tokens, norm_gain, gate_trained, up_trained, down_trained
    )
    mixed = scatter_sum(own, far, fs_count)
    return (*put_out(land, land_down), mixed)


def per_device_plain(tokens, norm_gain, gate_trained, up_trained, down_trained):
    gate_local = (norm_gain[:, None] * gate_trained).astype(jnp.bfloat16)
    up_local = (norm_gain[:, None] * up_trained).astype(jnp.bfloat16)
    down_local = down_trained.astype(jnp.bfloat16)
    tp_count = lax.axis_size("tp")
    fs_count = lax.axis_size("fs")
    rows_local = gate_local.shape[0]
    cols_local = gate_local.shape[1]
    model_width = rows_local * fs_count
    owned_count = cols_local * tp_count // fs_count
    piece_cols = owned_count // tp_count
    block_count = cols_local // owned_count

    def arrange(matrix):
        return matrix.reshape(rows_local, block_count, tp_count, piece_cols)

    gate_mixed, up_mixed = (
        lax.all_to_all(arrange(gate_local), "tp", split_axis=2, concat_axis=2, tiled=True),
        lax.all_to_all(arrange(up_local), "tp", split_axis=2, concat_axis=2, tiled=True),
    )

    def regroup(matrix):
        return matrix.transpose(2, 1, 0, 3).reshape(fs_count, rows_local, piece_cols)

    gate_parts, up_parts = (
        lax.all_to_all(regroup(gate_mixed), "fs", split_axis=0, concat_axis=1, tiled=True),
        lax.all_to_all(regroup(up_mixed), "fs", split_axis=0, concat_axis=1, tiled=True),
    )
    gate_sampler, up_sampler, down_sampler = (
        lax.all_gather(gate_parts.reshape(model_width, piece_cols), "tp", axis=1, tiled=True),
        lax.all_gather(up_parts.reshape(model_width, piece_cols), "tp", axis=1, tiled=True),
        lax.all_gather(down_local, "tp", axis=1, tiled=True),
    )
    as_float = tokens.astype(jnp.float32)
    normed = (
        as_float * lax.rsqrt(jnp.mean(as_float * as_float, axis=-1, keepdims=True) + 1e-06)
    ).astype(jnp.bfloat16)
    gate_act = jnp.dot(normed, gate_sampler, preferred_element_type=jnp.float32)
    up_act = jnp.dot(normed, up_sampler, preferred_element_type=jnp.float32)
    hidden = (jax.nn.silu(gate_act) * up_act).astype(jnp.bfloat16)
    partial_terms = jnp.dot(hidden, down_sampler, preferred_element_type=jnp.float32)
    mixed_out = lax.psum_scatter(partial_terms, "fs", scatter_dimension=1, tiled=True).astype(
        jnp.bfloat16
    )
    return (gate_sampler, up_sampler, down_sampler, mixed_out)


def solution(mesh):
    fs_count, tp_count = mesh.shape["fs"], mesh.shape["tp"]

    def body(tokens, norm_gain, gate_trained, up_trained, down_trained):
        rows, cols = gate_trained.shape
        aligned = (
            tp_count == 4
            and fs_count == 2 * tp_count == 8
            and rows % 256 == 0
            and (cols * tp_count // fs_count) % 128 == 0
            and (down_trained.shape[1] * tp_count // fs_count) % 128 == 0
            and down_trained.shape[0] % 64 == 0
            and tokens.shape[0] % 16 == 0
        )
        run = per_device if aligned else per_device_plain
        return run(tokens, norm_gain, gate_trained, up_trained, down_trained)

    in_specs = (P("tp", None), P("fs"), P("fs", "tp"), P("fs", "tp"), P("fs", "tp"))
    out_specs = (P(None, "fs"), P(None, "fs"), P("fs", None), P("tp", "fs"))
    return jax.shard_map(
        body, mesh=mesh, in_specs=in_specs, out_specs=out_specs, check_vma=False
    )
```

```python
import functools

import jax
import jax.numpy as jnp
from jax import lax
from jax.experimental import pallas as pl
from jax.experimental.pallas import tpu as pltpu
from jax.sharding import PartitionSpec as P

MESH = pl.DeviceIdType.MESH


def sent_terms(fs_count):
    half = fs_count // 2
    return [k for k in [*range(half, fs_count), *range(1, half)] if k not in paired(fs_count)]


def paired(fs_count):
    return [fs_count - 1 - 2 * i for i in range(2)]


def handoff_kernel(
    slabs, fs_count, tp_count, chunks,
    gain_ref, tokens_ref, gate_in, up_in, down_in, *refs,
):
    land, land_down, own_out, refs = refs[0], refs[1], refs[2], refs[3:]
    sent, pairs = sent_terms(fs_count), paired(fs_count)
    far_outs, refs = refs[:len(sent)], refs[len(sent):]
    (
        own, stage, fbuf, dbuf, normed, act, hidden, far_buf, gains,
        pair_buf, pair_in, pair_send, pair_recv,
        fetch_sem, down_sem, token_sem, swap_send, swap_recv, own_send, pass_send, recv,
        core_send, core_recv, cross_send, cross_recv, dx_send, dx_recv, dc_send, dc_recv,
        dp_send, dp_recv,
    ) = refs
    ins = (gate_in, up_in)
    blocks, _, rows, owned = own.shape
    down_rows, down_cols = dbuf.shape[1], down_in.shape[1]
    side = fs_count // 2
    cut = rows // 2
    count = len(slabs)
    early = [p for p in range(count) if slabs[p][0] < cut]
    late = [p for p in range(count) if slabs[p][0] >= cut]

    f = lax.axis_index("fs")
    t = lax.axis_index("tp")
    plane, core = lax.div(t, 2), lax.rem(t, 2)
    across = plane * -2 + 2 + core
    partner = plane * 2 + 1 - core
    far_partner = plane * -2 + 3 - core
    z = lax.div(f, blocks)
    half = lax.div(f, side)
    native = half == plane
    foreign = jnp.logical_not(native)
    held_here = lax.rem(z, 2) == core

    def some(condition, body, *args):
        pl.when(condition)(functools.partial(body, *args))

    def remote(src, dst, send, sem, to):
        return pltpu.make_async_remote_copy(
            src_ref=src, dst_ref=dst, send_sem=send, recv_sem=sem, device_id=to,
            device_id_type=MESH,
        )

    def at(m, source, start, size):
        return land.at[m, pl.ds(pl.multiple_of(source * rows + start, 16), size), :]

    def columns(p):
        first = lax.rem(z + p, blocks)
        return [lax.rem(first + k, blocks) for k in range(blocks)]

    def key(p, j, m):
        return p * blocks * 2 + j * 2 + m

    def group(p, within):
        if p in late:
            return p - 1
        return jnp.where(within, 0, p // 2)

    def cuts(p):
        start, size = slabs[p]
        if p != 1 or size <= 32:
            return [(start, size)]
        return [(start, 32), (start + 32, size - 32)]

    def swap(p, j, m, n=0):
        there = pl.ds(*cuts(p)[n])
        return remote(
            own.at[j, m, there, :], stage.at[j, m, there, :],
            swap_send.at[key(0, j, m)], swap_recv.at[key(count if n else p, j, m)], (f, across),
        )

    def local_to(target, j, m):
        return jnp.logical_and(target * blocks + j == f, core == m)

    def send_to_owner(held, sems, target, within, p, j, m, piece=None):
        start, size = piece or slabs[p]
        there = remote(
            held.at[j, m, pl.ds(start, size), :], at(m, f, start, size),
            sems.at[key(0, j, m)], recv.at[f, group(p, within)],
            (target * blocks + j, plane * 2 + m),
        )
        local = local_to(target, j, m)

        @pl.when(local)
        def _():
            @pl.loop(0, size // 16)
            def _(i):
                src = pl.ds(pl.multiple_of(start + i * 16, 16), 16)
                dst = pl.ds(pl.multiple_of(f * rows + start + i * 16, 16), 16)
                land[m, dst, :] = held[j, m, src, :]

        pl.when(jnp.logical_not(local))(there.start)

    def wait_sent(held, sems, target, size, j, m):
        there = held.at[j, m, pl.ds(0, size), :]
        done = remote(there, there, sems.at[key(0, j, m)], recv.at[f, 0], (f, across))
        pl.when(jnp.logical_not(local_to(target, j, m)))(done.wait_send)

    steps = [(p, m) for p in range(count) for m in range(2)]
    depth = fbuf.shape[0]

    def fetch(k):
        p, m = steps[k]
        start, size = slabs[p]
        return pltpu.make_async_copy(
            ins[m].at[pl.ds(start, size), :], fbuf.at[k % depth, pl.ds(0, size), :],
            fetch_sem.at[k % depth],
        )

    def down_fetch(q):
        return pltpu.make_async_copy(
            down_in.at[pl.ds(q * down_rows, down_rows), :], dbuf.at[q % 2], down_sem.at[q % 2]
        )

    def begin(p, m):
        for j in columns(p):
            def crossing(j=j):
                swap(p, j, m).start()

            if len(cuts(p)) > 1:
                continue

            def direct(j=j):
                send_to_owner(own, own_send, t, native, p, j, m)

            if p == 0:
                direct()
                pl.when(native)(crossing)
            elif p == 1:
                crossing()
                pl.when(native)(direct)
            else:
                crossing()

        if len(cuts(p)) > 1:
            for n in range(2):
                for j in columns(p):
                    swap(p, j, m, n).start()

            @pl.when(native)
            def _():
                for j in columns(p):
                    send_to_owner(own, own_send, t, native, p, j, m)

    for k in range(depth):
        fetch(k).start()
    token_copy = pltpu.make_async_copy(tokens_ref, normed, token_sem)
    token_copy.start()
    barrier = pltpu.get_barrier_semaphore()
    width_of_plane = tp_count // 2
    peers = fs_count * width_of_plane
    place = f * width_of_plane + core

    @pl.loop(1, peers)
    def _(i):
        peer = lax.rem(place + i, peers)
        pl.semaphore_signal(
            barrier, inc=1, device_id_type=MESH,
            device_id=(
                lax.div(peer, width_of_plane),
                plane * width_of_plane + lax.rem(peer, width_of_plane),
            ),
        )

    pl.semaphore_signal(barrier, inc=1, device_id=(f, across), device_id_type=MESH)
    for g in range(rows // 128):
        row = gain_ref[0:1, g * 128:(g + 1) * 128]
        gains[g * 128:(g + 1) * 128, :] = jnp.broadcast_to(row, (128, 128)).T
    for k, (p, m) in enumerate(steps):
        start, size = slabs[p]
        fetch(k).wait()

        @pl.loop(0, size // 16)
        def _(i):
            src = pl.ds(pl.multiple_of(i * 16, 16), 16)
            dst = pl.ds(pl.multiple_of(start + i * 16, 16), 16)
            gain = gains[dst, 0:1]
            for j in range(blocks):
                own[j, m, dst, :] = (
                    gain * fbuf[k % depth, src, j * owned:(j + 1) * owned]
                ).astype(jnp.bfloat16)

        if k + depth < len(steps):
            fetch(k + depth).start()
        if k == 2:
            pl.semaphore_wait(barrier, peers)
            begin(*steps[0])
        if k >= 2:
            begin(*steps[k - 1])
    for q in range(min(2, chunks)):
        down_fetch(q).start()
    begin(*steps[-1])

    def down_at(which, q):
        return land_down.at[
            pl.ds(q * down_rows, down_rows),
            pl.ds(pl.multiple_of(which * down_cols, 128), down_cols),
        ]

    for q in range(chunks):
        down_fetch(q).wait()

        @pl.loop(0, down_rows // 16)
        def _(i):
            src = pl.ds(pl.multiple_of(i * 16, 16), 16)
            dst = pl.ds(pl.multiple_of(q * down_rows + i * 16, 16), 16)
            land_down[dst, pl.ds(pl.multiple_of(t * down_cols, 128), down_cols)] = (
                dbuf[q % 2, src, :].astype(jnp.bfloat16)
            )

        if q + 2 < chunks:
            down_fetch(q + 2).start()

    token_copy.wait()

    @pl.loop(0, normed.shape[0] // 16)
    def _(i):
        dst = pl.ds(pl.multiple_of(i * 16, 16), 16)
        value = normed[dst, :].astype(jnp.float32)
        scale = lax.rsqrt(jnp.mean(value * value, axis=-1, keepdims=True) + 1e-06)
        normed[dst, :] = (value * scale).astype(jnp.bfloat16)
        for m in range(2):
            act[m, dst, :] = jnp.zeros((16, owned), jnp.float32)

    def other(i):
        return (1 - half) * side + lax.rem(f + i, side)

    def same(i):
        return half * side + lax.rem(f + i, side)

    def to_partner(source, p):
        here = at(core, source, *slabs[p])
        return remote(
            here, here, core_send, core_recv.at[source, int(p in late)], (f, partner)
        )

    def wait_partner(source, which):
        here = at(1 - core, source, which * cut, cut)
        remote(here, here, core_send, core_recv.at[source, which], (f, partner)).wait_recv()

    def wait_arrived(source, which, start, size):
        here = at(core, source, start, size)
        remote(here, here, core_send, recv.at[source, which], (f, partner)).wait_recv()

    def crossed(source, p):
        here = at(core, source, *slabs[p])
        return remote(here, here, cross_send, cross_recv.at[source], (f, across))

    def cross_near(p):
        @pl.loop(0, side)
        def _(i):
            source = other(i)
            wait_arrived(source, 0, *slabs[p])
            crossed(source, p).start()
            to_partner(source, p).start()

    def take_far(p):
        @pl.loop(0, side)
        def _(i):
            source = other(i)
            crossed(source, p).wait_recv()
            to_partner(source, p).start()

    def down_cross(q):
        return remote(down_at(t, q), down_at(t, q), dx_send, dx_recv.at[q], (f, across))

    def down_core(which, q):
        return remote(
            down_at(which, q), down_at(which, q), dc_send, dc_recv.at[q], (f, partner)
        )

    def down_pass(which, q):
        return remote(
            down_at(which, q), down_at(which, q), dp_send, dp_recv.at[q], (f, partner)
        )

    def forward(p):
        for m in range(2):
            for n, piece in enumerate(cuts(p)):
                for j in columns(p):
                    swap(p, j, m, n).wait_recv()
                    send_to_owner(stage, pass_send, across, foreign, p, j, m, piece)

    turn = 3
    for p in range(count):
        if p == 0:
            pl.when(foreign)(functools.partial(forward, p))
        else:
            forward(p)
        if 2 + p < count:
            for j in columns(2 + p):
                for m in range(2):
                    send_to_owner(own, own_send, t, native, 2 + p, j, m)
        if p == turn:
            some(native, cross_near, 0)
            some(foreign, cross_near, 1)
            for q in range(chunks):
                down_cross(q).start()
                down_core(t, q).start()

    def take(source, p, which):
        wait_arrived(source, which, *slabs[p])
        to_partner(source, p).start()

    def take_within(source, ps, which):
        @pl.when(jnp.logical_not(jnp.logical_and(source == f, held_here)))
        def _():
            start = slabs[ps[0]][0]
            wait_arrived(source, which, start, sum(slabs[p][1] for p in ps))

        for p in ps:
            to_partner(source, p).start()

    def multiply(source, lo, size):
        lanes = pl.ds(pl.multiple_of(source * rows + lo, 128), size)
        left = normed[:, lanes]
        for m in range(2):
            act[m] += jnp.dot(
                left, land[m, pl.ds(pl.multiple_of(source * rows + lo, 16), size), :],
                preferred_element_type=jnp.float32,
            )

    @pl.loop(0, side)
    def _(i):
        take_within(same(i), early, 0)

    @pl.loop(0, side)
    def _(i):
        take(other(i), 2, 1)

    some(native, take_far, 1)
    some(foreign, take_far, 0)

    @pl.loop(0, fs_count)
    def _(i):
        source = lax.rem(half * side + i, fs_count)
        wait_partner(source, 0)
        multiply(source, 0, cut)

    def down_on(q):
        down_in_here = remote(
            down_at(across, q), down_at(across, q), dx_send, dx_recv.at[q], (f, across)
        )
        down_in_here.wait_recv()
        down_pass(across, q).start()

    def down_done(q):
        down_core(partner, q).wait_recv()
        down_pass(far_partner, q).wait_recv()

    for n, p in enumerate(late[:-1]):
        @pl.loop(0, side)
        def _(i):
            take_within(same(i), [p], p - 1)

        @pl.loop(0, side)
        def _(i):
            take(other(i), p, p - 1)

        if n < chunks - 2:
            down_on(n)
        if 0 < n < chunks - 2:
            down_done(n - 1)
    last_p = late[-1]

    def finish(source):
        wait_partner(source, 1)
        multiply(source, cut, rows - cut)

    @pl.loop(0, side)
    def _(i):
        take_within(same(i), [last_p], last_p - 1)

    @pl.loop(0, side)
    def _(i):
        finish(same(i))

    for q in range(chunks - 2, chunks - 1):
        down_on(q)
        down_done(q - 1)

    @pl.loop(0, side)
    def _(i):
        take(other(i), last_p, last_p - 1)

        @pl.when(i > 0)
        def _():
            finish(other(i - 1))

    for q in range(max(0, chunks - 1), chunks):
        down_on(q)
    finish(other(side - 1))
    down_done(chunks - 2)

    @pl.loop(0, normed.shape[0] // 16)
    def _(i):
        dst = pl.ds(pl.multiple_of(i * 16, 16), 16)
        gate = act[0, dst, :]
        small = jnp.exp(-jnp.abs(gate))
        silu = gate * jnp.where(gate >= 0, 1.0, small) / (1.0 + small)
        hidden[dst, :] = (silu * act[1, dst, :]).astype(jnp.bfloat16)

    down_done(chunks - 1)
    width = own_out.shape[1]

    def peer(k):
        return sum(lax.rem(lax.div(f, n) + k // n, 2) * n for n in (1, 2, 4))

    def term(b):
        lanes = pl.ds(pl.multiple_of(b * width, 128), width)
        return jnp.dot(hidden[...], land_down[:, lanes], preferred_element_type=jnp.float32)

    def keep(k, value):
        far_outs[sent.index(k)][...] = value.astype(jnp.bfloat16)

    def to_pair(i):
        return remote(
            far_buf.at[i], pair_in.at[i], pair_send.at[i], pair_recv.at[i], (peer(1), t)
        )

    for i, k in enumerate(pairs):
        far_buf[i] = term(peer(k)).astype(jnp.bfloat16)
        if i:
            to_pair(i - 1).start()
    summed = [k - 1 for k in pairs]
    for i, k in enumerate(summed):
        pair_buf[i] = term(peer(k))
        if i == 0:
            to_pair(len(pairs) - 1).start()
    for k in sent:
        if k not in summed:
            keep(k, term(peer(k)))
    own_out[...] = term(f)
    for i, k in enumerate(summed):
        to_pair(i).wait_recv()
        keep(k, pair_buf[i] + pair_in[i].astype(jnp.float32))

    def wait_kept(crossing, direct, passed):
        for j in range(blocks):
            for m in range(2):
                there = own.at[j, m, pl.ds(0, crossing), :]
                remote(
                    there, there, swap_send.at[key(0, j, m)], swap_recv.at[0], (f, across)
                ).wait_send()
                wait_sent(own, own_send, t, direct, j, m)
                wait_sent(stage, pass_send, across, passed, j, m)

    def wait_crossed(p):
        here = land.at[0, pl.ds(0, side * slabs[p][1]), :]
        remote(here, here, cross_send, cross_recv.at[0], (f, across)).wait_send()

    first, second = slabs[0][1], slabs[1][1]
    some(native, wait_kept, rows, rows, rows - first)
    some(foreign, wait_kept, rows - first, rows - second, rows)
    some(native, wait_crossed, 0)
    some(foreign, wait_crossed, 1)
    remote(land.at[core], land.at[core], core_send, recv.at[0, 0], (f, partner)).wait_send()
    whole = land_down.at[:, pl.ds(0, down_cols)]
    for sem in (dx_send, dc_send, dp_send):
        remote(whole, whole, sem, dx_recv.at[0], (f, partner)).wait_send()
    for i in range(len(pairs)):
        to_pair(i).wait_send()


def row_slabs(rows):
    first = max(16, (rows * 7 // 32) // 16 * 16)
    second = max(16, (rows * 7 // 32) // 16 * 16)
    cut = rows // 2
    slabs = [(0, first), (first, second), (first + second, cut - first - second)]
    left, start = (rows - cut) // 16, cut
    final = max(1, left // 8)
    third = max(1, left * 3 // 16)
    front = left - final - third
    for units in (front - front // 2, front // 2, third, final):
        slabs.append((start, units * 16))
        start += units * 16
    return slabs


def handoff(fs_count, tp_count, chunks, tokens, norm_gain, gate, up, down):
    rows, cols = gate.shape
    blocks = fs_count // tp_count
    owned = cols // blocks
    width = down.shape[1] * tp_count // fs_count
    down_rows, down_cols = down.shape
    model = rows * fs_count
    count = tokens.shape[0]
    slabs = row_slabs(rows)
    parts = len(slabs)
    f32, bf16, dma = jnp.float32, jnp.bfloat16, pltpu.SemaphoreType.DMA
    anywhere = pl.BlockSpec(memory_space=pl.ANY)
    inside = pl.BlockSpec(memory_space=pltpu.VMEM)
    tall = max(size for _, size in slabs)
    pieces = (parts + 1) * blocks * 2
    pairs = len(paired(fs_count))
    return pl.pallas_call(
        functools.partial(handoff_kernel, slabs, fs_count, tp_count, chunks),
        out_shape=[
            pltpu.VMEM((2, model, owned), bf16),
            pltpu.VMEM((down_rows, down_cols * tp_count), bf16),
            pltpu.VMEM((count, width), f32),
        ] + [pltpu.VMEM((count, width), bf16)] * len(sent_terms(fs_count)),
        in_specs=[inside] + [anywhere] * 4,
        out_specs=[inside] * (3 + len(sent_terms(fs_count))),
        scratch_shapes=[
            pltpu.VMEM((blocks, 2, rows, owned), bf16),
            pltpu.VMEM((blocks, 2, rows, owned), bf16),
            pltpu.VMEM((3, tall, cols), f32),
            pltpu.VMEM((2, down_rows // chunks, down_cols), f32),
            pltpu.VMEM(tokens.shape, bf16),
            pltpu.VMEM((2, count, owned), f32),
            pltpu.VMEM((count, owned), bf16),
            pltpu.VMEM((pairs, count, width), bf16),
            pltpu.VMEM((rows, 128), f32),
            pltpu.VMEM((pairs, count, width), f32), pltpu.VMEM((pairs, count, width), bf16),
            dma((pairs,)), dma((pairs,)),
            dma((3,)), dma((2,)), dma(()),
            dma((blocks * 2,)), dma((pieces,)), dma((blocks * 2,)), dma((blocks * 2,)),
            dma((fs_count, parts - 1)), dma(()), dma((fs_count, 2)),
            dma(()), dma((fs_count,)),
            dma(()), dma((chunks,)), dma(()), dma((chunks,)), dma(()), dma((chunks,)),
        ],
        compiler_params=pltpu.CompilerParams(
            collective_id=0, has_side_effects=True, vmem_limit_bytes=27 * 1024 * 1024
        ),
    )(norm_gain[None, :], tokens, gate, up, down)


def put_out(land, land_down):
    def copy_kernel(land_ref, down_ref, gate_ref, up_ref, down_out_ref, sems):
        copies = []
        for source, target in ((land_ref.at[0], gate_ref), (land_ref.at[1], up_ref), (down_ref, down_out_ref)):
            tall = target.shape[0] // 8
            for k in range(8):
                here = pl.ds(k * tall, tall)
                copies.append(pltpu.make_async_copy(source.at[here, :], target.at[here, :], sems.at[len(copies)]))
        for c in copies:
            c.start()
        for c in copies:
            c.wait()

    anywhere = pl.BlockSpec(memory_space=pl.ANY)
    inside = pl.BlockSpec(memory_space=pltpu.VMEM)
    return pl.pallas_call(
        copy_kernel,
        out_shape=[
            jax.ShapeDtypeStruct(land.shape[1:], land.dtype),
            jax.ShapeDtypeStruct(land.shape[1:], land.dtype),
            jax.ShapeDtypeStruct(land_down.shape, land_down.dtype),
        ],
        in_specs=[inside] * 2,
        out_specs=[anywhere] * 3,
        scratch_shapes=[pltpu.SemaphoreType.DMA((24,))],
        compiler_params=pltpu.CompilerParams(vmem_limit_bytes=27 * 1024 * 1024),
        cost_estimate=pl.CostEstimate(
            flops=0, bytes_accessed=4 * (land.size + land_down.size), transcendentals=0
        ),
    )(pltpu.with_memory_space_constraint(land, pltpu.VMEM), pltpu.with_memory_space_constraint(land_down, pltpu.VMEM))


def scatter_sum(own, far, fs_count):
    arrived = []
    for k, sent in zip(sent_terms(fs_count), far):
        ring = [(i, i ^ k) for i in range(fs_count)]
        arrived.append(lax.ppermute(sent, "fs", ring))
    total = own
    for piece in arrived:
        total = total + piece.astype(jnp.float32)
    return total.astype(jnp.bfloat16)


def per_device(tokens, norm_gain, gate_trained, up_trained, down_trained):
    tp_count = lax.axis_size("tp")
    fs_count = lax.axis_size("fs")
    land, land_down, own, *far = handoff(
        fs_count, tp_count, 4, tokens, norm_gain, gate_trained, up_trained, down_trained
    )
    mixed = scatter_sum(own, far, fs_count)
    return (*put_out(land, land_down), mixed)


def per_device_plain(tokens, norm_gain, gate_trained, up_trained, down_trained):
    gate_local = (norm_gain[:, None] * gate_trained).astype(jnp.bfloat16)
    up_local = (norm_gain[:, None] * up_trained).astype(jnp.bfloat16)
    down_local = down_trained.astype(jnp.bfloat16)
    tp_count = lax.axis_size("tp")
    fs_count = lax.axis_size("fs")
    rows_local = gate_local.shape[0]
    cols_local = gate_local.shape[1]
    model_width = rows_local * fs_count
    owned_count = cols_local * tp_count // fs_count
    piece_cols = owned_count // tp_count
    block_count = cols_local // owned_count

    def arrange(matrix):
        return matrix.reshape(rows_local, block_count, tp_count, piece_cols)

    gate_mixed, up_mixed = (
        lax.all_to_all(arrange(gate_local), "tp", split_axis=2, concat_axis=2, tiled=True),
        lax.all_to_all(arrange(up_local), "tp", split_axis=2, concat_axis=2, tiled=True),
    )

    def regroup(matrix):
        return matrix.transpose(2, 1, 0, 3).reshape(fs_count, rows_local, piece_cols)

    gate_parts, up_parts = (
        lax.all_to_all(regroup(gate_mixed), "fs", split_axis=0, concat_axis=1, tiled=True),
        lax.all_to_all(regroup(up_mixed), "fs", split_axis=0, concat_axis=1, tiled=True),
    )
    gate_sampler, up_sampler, down_sampler = (
        lax.all_gather(gate_parts.reshape(model_width, piece_cols), "tp", axis=1, tiled=True),
        lax.all_gather(up_parts.reshape(model_width, piece_cols), "tp", axis=1, tiled=True),
        lax.all_gather(down_local, "tp", axis=1, tiled=True),
    )
    as_float = tokens.astype(jnp.float32)
    normed = (
        as_float * lax.rsqrt(jnp.mean(as_float * as_float, axis=-1, keepdims=True) + 1e-06)
    ).astype(jnp.bfloat16)
    gate_act = jnp.dot(normed, gate_sampler, preferred_element_type=jnp.float32)
    up_act = jnp.dot(normed, up_sampler, preferred_element_type=jnp.float32)
    hidden = (jax.nn.silu(gate_act) * up_act).astype(jnp.bfloat16)
    partial_terms = jnp.dot(hidden, down_sampler, preferred_element_type=jnp.float32)
    mixed_out = lax.psum_scatter(partial_terms, "fs", scatter_dimension=1, tiled=True).astype(
        jnp.bfloat16
    )
    return (gate_sampler, up_sampler, down_sampler, mixed_out)


def solution(mesh):
    fs_count, tp_count = mesh.shape["fs"], mesh.shape["tp"]

    def body(tokens, norm_gain, gate_trained, up_trained, down_trained):
        rows, cols = gate_trained.shape
        aligned = (
            tp_count == 4
            and fs_count == 2 * tp_count == 8
            and rows % 256 == 0
            and (cols * tp_count // fs_count) % 128 == 0
            and (down_trained.shape[1] * tp_count // fs_count) % 128 == 0
            and down_trained.shape[0] % 64 == 0
            and tokens.shape[0] % 16 == 0
        )
        run = per_device if aligned else per_device_plain
        return run(tokens, norm_gain, gate_trained, up_trained, down_trained)

    in_specs = (P("tp", None), P("fs"), P("fs", "tp"), P("fs", "tp"), P("fs", "tp"))
    out_specs = (P(None, "fs"), P(None, "fs"), P("fs", None), P("tp", "fs"))
    return jax.shard_map(
        body, mesh=mesh, in_specs=in_specs, out_specs=out_specs, check_vma=False
    )
```
